512 devices in a mesh: sp: 128 (over z, y, core), tp: 4 (over x).
Axes of the slice: x: 4, y: 8, z: 8, core: 2. Of those that a mesh axis runs over, the one named last changes fastest.
Arguments:
- tokens: bfloat16 [65536, 2048], P(('sp', 'tp')), may hold values from -6 to 6
- norm_gain: bfloat16 [2048], replicated, may hold values from 0.099609375 to 1.8984375
- proj_x: bfloat16 [2048, 2048], P('sp', 'tp'), may hold values from -0.125 to 0.125
- gate_projection: bfloat16 [2048, 2048], P('sp', 'tp'), may hold values from -0.125 to 0.125
- conv_taps: bfloat16 [4, 2048], P(None, 'tp'), may hold values from -3 to 3
- gate_recur: bfloat16 [8, 256, 256], P('tp'), may hold values from -0.375 to 0.375
- gate_input: bfloat16 [8, 256, 256], P('tp'), may hold values from -0.375 to 0.375
- decay_param: float32 [2048], P('tp'), may hold values from 4 to 25
- decay_shift: float32 [8, 65536], P('tp', 'sp'), may hold values from -1.3 to 0, as said below
- proj_out: bfloat16 [2048, 2048], P('tp', 'sp'), may hold values from -0.125 to 0.125
Outputs:
- mixed_out: bfloat16 [65536, 2048], P(('sp', 'tp'))
The draws below stay inside these ranges and needn't reach their ends.
Inputs may be any that keep to these rules, and one draw needn't show every extreme that they name: `decay_shift`: added log-decays, never positive.
All inputs are finite; a program needn't handle non-finite values.
Results may differ from the reference program's by a relative error of at most 0.015.
Values may be sent and summed in bfloat16 or wider, within the bound.
A program may use at most 128 MiB of HBM per device.

```python
import jax
import jax.numpy as jnp
from jax import lax

D = 2048
WIDTH = 2048
HEAD = 256
CONV = 4
GROUP = 512
SEQ = 65536
N_TP = 4


def draw_decay_param(key, part):
    key_pick, key_slow, key_fast = jax.random.split(jax.random.fold_in(key, 11), 3)
    fast_share = 0.5
    picked = jax.random.uniform(key_pick, (WIDTH,), jnp.float32) < fast_share
    slow_rate = jnp.exp(jax.random.uniform(key_slow, (WIDTH,), jnp.float32, jnp.log(0.1), jnp.log(0.6))) / (8.0 * SEQ)
    fast_rate = jnp.exp(jax.random.uniform(key_fast, (WIDTH,), jnp.float32, jnp.log(0.0025), jnp.log(0.0083)))
    chosen = jnp.where(picked, fast_rate, slow_rate)
    return -jnp.log(jnp.expm1(chosen))


def draw_decay_shift(key, part):
    key_base, key_where, key_size = jax.random.split(jax.random.fold_in(key, 23), 3)
    head_count = WIDTH // HEAD
    block_count = SEQ // GROUP
    base = jnp.exp(jax.random.uniform(key_base, (block_count,), jnp.float32, jnp.log(0.05), jnp.log(0.3))) / SEQ
    starting_rows = jnp.repeat(base, GROUP)
    target_slots = jax.random.randint(key_where, (head_count, 2), 0, SEQ)
    segment_sizes = jax.random.uniform(key_size, (head_count, 2), jnp.float32, 0.22, 0.6)
    token_offsets = jnp.arange(SEQ)
    token_runs = jnp.sum(jnp.where(token_offsets[None, None, :] == target_slots[:, :, None], segment_sizes[:, :, None], 0.0), axis=1)
    return -(starting_rows[None, :] + token_runs)


def shard_levels(own_key, extent, pieces, least, largest):
    factor_of = 1.0
    for position, blocks in pieces:
        draws = jax.random.uniform(jax.random.fold_in(jax.random.fold_in(own_key, 6), position), (blocks,), jnp.float32, least / len(pieces), largest / len(pieces))
        factor_of = factor_of * jnp.repeat(jnp.exp(draws), extent[position] // blocks).reshape((-1,) + (1,) * (len(extent) - 1 - position))
    return factor_of


def normal_values(stream_key, extent, spread, limit, cuts=(), kind=jnp.bfloat16):
    result = spread * jax.random.normal(stream_key, extent, jnp.float32)
    if cuts:
        result = result * shard_levels(stream_key, extent, cuts, -0.22, 0.18)
    return jnp.clip(result, -limit, limit).astype(kind)


def setup_inputs(seed: int = 0) -> dict:
    key_list = jax.random.split(jax.random.key(seed), 11)
    return {
        "tokens": normal_values(key_list[0], (SEQ, D), 1.0, 6.0, ((0, 512),)),
        "norm_gain": jnp.clip(1.0 + 0.18 * jax.random.normal(key_list[1], (D,), jnp.float32), 0.099609375, 1.8984375).astype(jnp.bfloat16),
        "proj_x": normal_values(key_list[2], (D, WIDTH), D ** -0.5, 0.125, ((0, 128), (1, 4))),
        "gate_projection": normal_values(key_list[3], (D, WIDTH), D ** -0.5, 0.125, ((0, 128), (1, 4))),
        "conv_taps": normal_values(key_list[4], (CONV, WIDTH), CONV ** -0.5, 3.0, ((1, 4),)),
        "gate_recur": normal_values(key_list[5], (WIDTH // HEAD, HEAD, HEAD), HEAD ** -0.5, 0.375, ((0, 4),)),
        "gate_input": normal_values(key_list[6], (WIDTH // HEAD, HEAD, HEAD), HEAD ** -0.5, 0.375, ((0, 4),)),
        "decay_param": draw_decay_param(jax.random.fold_in(key_list[10], 71), 0),
        "decay_shift": draw_decay_shift(jax.random.fold_in(key_list[10], 71), 0),
        "proj_out": normal_values(key_list[9], (WIDTH, D), WIDTH ** -0.5, 0.125, ((0, 4), (1, 128))),
    }


def rms_norm(values, norm_gain):
    floats = values.astype(jnp.float32)
    scaled = floats * lax.rsqrt(lax.optimization_barrier(jnp.mean(floats * floats, axis=-1, keepdims=True)) + 1e-06)
    return (scaled * norm_gain.astype(jnp.float32)).astype(jnp.bfloat16)

def combine_pair(earlier, later):
    return (earlier[0] * later[0], later[0] * earlier[1] + later[1])

def reference(tokens, norm_gain, proj_x, gate_projection, conv_taps, gate_recur, gate_input, decay_param, decay_shift, proj_out):
    block_count = SEQ // GROUP
    head_count = WIDTH // HEAD
    channel_block = WIDTH // N_TP
    token_blocks = tokens.reshape(block_count, GROUP, D)
    shift_blocks = jnp.transpose(decay_shift.reshape(head_count, block_count, GROUP), (1, 2, 0))
    decay_rate = jax.nn.softplus(-decay_param.astype(jnp.float32)).reshape(head_count, HEAD)

    def advance(carried, inputs):
        state_now, tail_rows = carried
        block_tokens, block_shift = inputs
        normed = rms_norm(block_tokens, norm_gain)
        branch = jnp.dot(normed, proj_x, preferred_element_type=jnp.float32).astype(jnp.bfloat16)
        gating = jnp.dot(normed, gate_projection, preferred_element_type=jnp.float32).astype(jnp.bfloat16)
        extended = jnp.concatenate([tail_rows, branch], axis=0)
        conv_sum = jnp.zeros((GROUP, WIDTH), jnp.float32)
        for tap_index in range(CONV):
            conv_sum = conv_sum + extended[tap_index:tap_index + GROUP].astype(jnp.float32) * conv_taps[tap_index].astype(jnp.float32)
        conved = conv_sum.astype(jnp.bfloat16)
        grouped = conved.reshape(GROUP, head_count, HEAD).astype(jnp.float32)
        recur = jax.nn.sigmoid(jnp.einsum('thi,hij->thj', grouped, gate_recur.astype(jnp.float32)))
        inlet = jax.nn.sigmoid(jnp.einsum('thi,hij->thj', grouped, gate_input.astype(jnp.float32)))
        log_decay = (-8.0 * recur * decay_rate[None] + block_shift[:, :, None]).reshape(GROUP, WIDTH)
        decay = jnp.exp(log_decay)
        drive = jnp.sqrt(-jnp.expm1(2.0 * log_decay)) * inlet.reshape(GROUP, WIDTH) * conved.astype(jnp.float32)
        drive = drive.at[0].add(decay[0] * state_now)
        states = lax.associative_scan(combine_pair, (decay, drive), axis=0)[1]
        mixed = (states * jax.nn.gelu(gating.astype(jnp.float32))).astype(jnp.bfloat16)
        total = jnp.zeros((GROUP, D), jnp.float32)
        for block_index in range(N_TP):
            lower = block_index * channel_block
            partial_out = jnp.dot(mixed[:, lower:lower + channel_block], proj_out[lower:lower + channel_block], preferred_element_type=jnp.float32).astype(jnp.bfloat16)
            total = total + lax.optimization_barrier(partial_out).astype(jnp.float32)
        return ((states[GROUP - 1], branch[GROUP - CONV + 1:]), total.astype(jnp.bfloat16))
    initial = (jnp.zeros((WIDTH,), jnp.float32), jnp.zeros((CONV - 1, WIDTH), jnp.bfloat16))
    unused, output_values = lax.scan(advance, initial, (token_blocks, shift_blocks))
    return output_values.reshape(SEQ, D)
```

```python
import functools

import jax
import jax.numpy as jnp
from jax import lax
from jax.experimental import pallas as pl
from jax.experimental.pallas import tpu as pltpu
from jax.sharding import Mesh
from jax.sharding import PartitionSpec as P

HEAD = 256
CONV = 4
SP = ("sp_0", "sp_1", "sp_2")
SP_TP = ("sp_0", "sp_1", "sp_2", "tp")
MESH = pl.DeviceIdType.MESH
F32 = jnp.float32
BF16 = jnp.bfloat16
LANES = 128


def body(
    nz, ny,
    tokens, gain, proj_x, gate_proj, taps, gate_recur, gate_input, decay_param, decay_shift, proj_out,
    out,
    tok, nrm, stage, wb, gr, gi, branch, dec, drv, shiftc, gel, mx, tail,
    mine1, s1, mine2, s2, cin, dummy, outv,
    po_far, po_next, po_prev, in_rel, in_prev, in_next,
    lsem, gsem, tsend, trecv, p1send, p1recv, rsend, rrecv, dsend, drecv, xsem, osend, orecv,
):
    z, y, c, x = (lax.axis_index(a) for a in SP_TP)
    t = tok.shape[1]
    half = t // 2
    rows = 4 * t
    chunk = rows // 8
    width = 2 * wb.shape[-1]
    groups = width // LANES
    heads = width // HEAD
    pw = width // 2
    nr = wb.shape[2]
    sp_index = (z * ny + y) * 2 + c
    sp_count = nz * ny * 2

    def at(dz=0, dy=0, dc=None, dx=0, core=None):
        cc = c if dc is None else lax.rem(c + dc, 2)
        cc = cc if core is None else core
        return {
            "sp_0": lax.rem(z + dz + nz, nz), "sp_1": lax.rem(y + dy + ny, ny),
            "sp_2": cc, "tp": lax.rem(x + dx + 4, 4),
        }

    def remote(src, dst, send, recv, where):
        return pltpu.make_async_remote_copy(
            src_ref=src, dst_ref=dst, send_sem=send, recv_sem=recv, device_id=where, device_id_type=MESH
        )

    right, left = lax.rem(x + 1, 4), lax.rem(x + 3, 4)
    far = lax.rem(x + 2, 4)

    nsp = lax.rem(sp_index + 1, sp_count)
    psp = lax.rem(sp_index + sp_count - 1, sp_count)

    def of_sp(s):
        return {"sp_0": s // (2 * ny), "sp_1": lax.rem(s // 2, ny), "sp_2": lax.rem(s, 2), "tp": x}

    own_tok = pltpu.make_async_copy(tokens, tok.at[x], lsem.at[0])
    own_tok.start()
    ring = z * (1 - c) + y * c
    cross = y * (1 - c) + z * c
    core_row = pl.multiple_of(c * 16, 16)
    core_col = pl.multiple_of(c * pw, pw)
    stage_loads = []
    for m, src in enumerate((proj_x, gate_proj, proj_out)):
        loads = []
        for p in range(2):
            loads.append(pltpu.make_async_copy(src.at[:, pl.ds(p * pw, pw)], stage.at[m, p], lsem.at[1 + 3 * m + p]))
        loads.append(pltpu.make_async_copy(
            src.at[:, pl.ds(core_col, pw)], wb.at[m, c, ring, cross, pl.ds(core_row, 16)], lsem.at[3 + 3 * m]))
        for load in loads:
            load.start()
        stage_loads.append(loads)
    gate_loads = [
        pltpu.make_async_copy(gate_recur, gr, gsem.at[0]),
        pltpu.make_async_copy(gate_input, gi, gsem.at[1]),
    ]
    for load in gate_loads:
        load.start()

    barrier = pltpu.get_barrier_semaphore()
    peers = [at(dx=1), at(dx=-1)]
    peers += [at(dc=1)]
    peers += [at(dy=k, dc=d) for k in range(1, ny) for d in range(2)]
    peers += [at(dz=k, dc=d) for k in range(1, nz) for d in range(2)]
    peers += [of_sp(nsp), of_sp(psp)]
    for peer in peers:
        pl.semaphore_signal(barrier, inc=1, device_id=peer, device_id_type=MESH)
    pl.semaphore_wait(barrier, len(peers))

    own_tok.wait()
    lo, hi = pl.ds(0, half), pl.ds(half, half)
    tok_a_r = remote(tok.at[x, lo], tok.at[x, lo], tsend.at[0], trecv.at[0], at(dx=1))
    tok_b_r = remote(tok.at[x, hi], tok.at[x, hi], tsend.at[1], trecv.at[1], at(dx=1))
    tok_b_l = remote(tok.at[x, hi], tok.at[x, hi], tsend.at[2], trecv.at[2], at(dx=-1))
    tok_a_l = remote(tok.at[x, lo], tok.at[x, lo], tsend.at[3], trecv.at[3], at(dx=-1))
    rel_a = remote(tok.at[left, lo], tok.at[left, lo], tsend.at[4], trecv.at[4], at(dx=1))
    rel_b = remote(tok.at[right, hi], tok.at[right, hi], tsend.at[5], trecv.at[5], at(dx=-1))
    for copy in (tok_a_r, tok_b_l, tok_b_r, tok_a_l):
        copy.start()

    def first_phase(m):
        for load in stage_loads[m]:
            load.wait()
        for k in range(1, ny):
            remote(stage.at[m, 0], wb.at[m, 0, z, y, pl.ds(core_row, 16)], p1send.at[m], p1recv.at[m],
                   at(dy=k, core=0)).start()
        for k in range(1, nz):
            remote(stage.at[m, 1], wb.at[m, 1, y, z, pl.ds(core_row, 16)], p1send.at[m], p1recv.at[m],
                   at(dz=k, core=1)).start()
        other = 1 - c
        r2 = z * c + y * (1 - c)
        q2 = y * c + z * (1 - c)
        remote(stage.at[m, other], wb.at[m, other, r2, q2, pl.ds(core_row, 16)], p1send.at[m], p1recv.at[m],
               at(dc=1)).start()

    def first_phase_done(m):
        pltpu.make_async_copy(dummy, dummy, p1recv.at[m]).wait()

    def ring_at(step):
        return {
            "sp_0": lax.rem(z + (1 - c) * step + nr, nr) * (1 - c) + z * c,
            "sp_1": lax.rem(y + c * step + nr, nr) * c + y * (1 - c),
            "sp_2": c, "tp": x,
        }

    last = nr // 2 - 1
    nq = wb.shape[3]

    def piece(step, way):
        if step < last:
            return pl.ds(0, nq)
        return pl.ds(0, nq // 2) if way == 0 else pl.ds(nq // 2, nq // 2)

    def ring_copy(m, way, step):
        sign = 1 if way == 0 else -1
        block = lax.rem(ring - sign * step + nr, nr)
        ref = wb.at[m, c, block, piece(step, way)]
        return remote(ref, ref, rsend.at[m, way, step], rrecv.at[m, way, step], ring_at(sign))

    def share(m, block, part):
        ref = wb.at[m, c, block, part]
        remote(ref, ref, dsend.at[m], drecv.at[m], at(dc=1)).start()

    def ring_first(m):
        first_phase_done(m)
        for way in range(2):
            ring_copy(m, way, 0).start()
        share(m, ring, pl.ds(0, nq))

    def ring_arrived(m, way, step):
        sign = 1 if way == 0 else -1
        ring_copy(m, way, step).wait_recv()
        if step < last:
            ring_copy(m, way, step + 1).start()
        share(m, lax.rem(ring - sign * (step + 1) + nr, nr), piece(step, way))

    def ring_step(m, step):
        for way in range(2):
            ring_arrived(m, way, step)

    def shared_done(m):
        whole = wb.at[m, 1 - c]
        pltpu.make_async_copy(whole, whole, drecv.at[m]).wait()

    def norm_block(b):
        g = gain[...].astype(F32)

        @pl.loop(0, t // 16)
        def _(i):
            r = pl.ds(pl.multiple_of(i * 16, 16), 16)
            v = tok[b, r, :].astype(F32)
            s = lax.rsqrt(jnp.mean(v * v, axis=-1, keepdims=True) + 1e-06)
            nrm[b, r, :] = (v * s * g).astype(BF16)

    def weight(m, p):
        if p == 0:
            return wb[m, 0].reshape(-1, pw)
        return jnp.concatenate([wb[m, 1, :, k].reshape(-1, pw) for k in range(nq)], axis=0)

    first_phase(0)
    first_phase(1)
    norm_block(x)

    for h in range(heads):
        for k in range(rows // LANES):
            line = decay_shift[h:h + 1, k * LANES:(k + 1) * LANES]
            shiftc[h, k * LANES:(k + 1) * LANES, :] = jnp.transpose(jnp.broadcast_to(line, (LANES, LANES)))
    v = jnp.exp(-decay_param[...])
    rate = v * (1.0 - v * (1 / 2 - v * (1 / 3 - v * (1 / 4 - v * (1 / 5)))))
    rate8 = -8.0 * rate

    ring_first(0)
    ring_first(1)
    first_phase(2)
    for step in range(last):
        ring_step(0, step)
        if step == 0:
            tok_a_r.wait_recv()
            rel_a.start()
            tok_b_l.wait_recv()
            rel_b.start()
        ring_step(1, step)
    ring_step(0, last)
    ring_step(1, last)
    ring_first(2)
    tok_b_r.wait_recv()
    tok_a_l.wait_recv()
    norm_block(left)
    norm_block(right)
    shared_done(0)

    def branch_block(b):
        at_row = pl.ds(pl.multiple_of(8 + b * t, 8), t)
        for p in range(2):
            prod = jnp.dot(nrm[b], weight(0, p), preferred_element_type=F32)
            branch[at_row, p * pw:(p + 1) * pw] = prod.astype(BF16).astype(F32)

    @pl.loop(0, 3)
    def _(k):
        branch_block(lax.rem(x + 3 + k, 4))

    ring_step(2, 0)
    rel_a.wait_recv()
    rel_b.wait_recv()
    norm_block(far)
    branch_block(far)

    tail_copy = remote(branch.at[pl.ds(rows, 8)], tail, xsem.at[0], xsem.at[1], of_sp(nsp))
    tail_copy.start()
    if last >= 1:
        ring_step(2, 1)
    for load in gate_loads:
        load.wait()

    tapf = taps[...].astype(F32)

    def gates(i):
        base = pl.multiple_of(i * t, t)
        win = branch[pl.ds(base, t + 8), :]
        acc = jnp.zeros((t, width), F32)
        for k in range(CONV):
            acc = acc + win[5 + k:5 + k + t] * tapf[k:k + 1]
        conv = acc.astype(BF16)
        at_row = pl.ds(base, t)
        for h in range(heads):
            cols = slice(h * HEAD, (h + 1) * HEAD)
            cb = conv[:, cols]
            cf = cb.astype(F32)
            ur = jnp.dot(cb, gr[h], preferred_element_type=F32)
            ui = jnp.dot(cb, gi[h], preferred_element_type=F32)
            recur = 1.0 / (1.0 + jnp.exp(-ur))
            inlet = 1.0 / (1.0 + jnp.exp(-ui))
            sh = shiftc[h, at_row, :]
            log_decay = recur * rate8[:, cols] + jnp.concatenate([sh] * (HEAD // LANES), axis=1)
            decay = jnp.exp(log_decay)
            u = 2.0 * log_decay
            near = u * (1.0 + u * (1 / 2) * (1.0 + u * (1 / 3) * (1.0 + u * (1 / 4) * (1.0 + u * (1 / 5) * (1.0 + u * (1 / 6))))))
            em1 = jnp.where(u > -0.25, near, decay * decay - 1.0)
            drive = jnp.sqrt(-em1) * inlet * cf
            for g in range(HEAD // LANES):
                lanes = slice(g * LANES, (g + 1) * LANES)
                dec[h * (HEAD // LANES) + g, at_row, :] = decay[:, lanes]
                drv[h * (HEAD // LANES) + g, at_row, :] = drive[:, lanes]

    @pl.loop(0, 3)
    def _(k):
        gates(3 - k)

    tail_copy.wait_recv()
    keep = jnp.where(sp_index > 0, 1.0, 0.0).astype(F32)
    branch[0:8, :] = tail[...] * keep
    gates(0)

    def scan_step(j, carried):
        pos = pl.ds(j, 8, stride=chunk)
        new = []
        for g in range(groups):
            prod, state = carried[g]
            a = dec[g, pos, :]
            b = drv[g, pos, :]
            state = a * state + b
            prod = prod * a
            dec[g, pos, :] = prod
            drv[g, pos, :] = state
            new.append((prod, state))
        return tuple(new)

    one, zero = jnp.ones((8, LANES), F32), jnp.zeros((8, LANES), F32)
    ends = lax.fori_loop(0, chunk, scan_step, ((one, zero),) * groups, unroll=4)
    for g in range(groups):
        prod, state = ends[g]
        pr, st = prod[0:1], state[0:1]
        for i in range(1, 8):
            st = prod[i:i + 1] * st + state[i:i + 1]
            pr = pr * prod[i:i + 1]
        mine1[0:1, g * LANES:(g + 1) * LANES] = pr
        mine1[1:2, g * LANES:(g + 1) * LANES] = st

    me1 = y * 2 + c
    n1 = 2 * ny
    firsts = [at(dc=1)] + [at(dy=k, dc=d) for k in range(1, ny) for d in range(2)]
    for peer in firsts:
        remote(mine1, s1.at[me1], xsem.at[2], xsem.at[3], peer).start()
    s1[me1] = mine1[...]

    def gating_block(b):
        for p in range(2):
            cols = slice(p * pw, (p + 1) * pw)
            prod = jnp.dot(nrm[b], weight(1, p), preferred_element_type=F32)
            v = prod.astype(BF16).astype(F32)
            inner = 0.7978845608028654 * (v + 0.044715 * (v * v * v))
            gel[pl.ds(pl.multiple_of(b * t, t), t), cols] = 0.5 * v * (1.0 + jnp.tanh(inner))

    shared_done(1)

    @pl.loop(0, 2)
    def _(b):
        gating_block(b)

    pltpu.make_async_copy(s1.at[pl.ds(0, n1 - 1)], s1.at[pl.ds(0, n1 - 1)], xsem.at[3]).wait()
    p_all, s_all = s1[0, 0:1], s1[0, 1:2]
    p_in = jnp.where(me1 > 0, p_all, 1.0)
    s_in = jnp.where(me1 > 0, s_all, 0.0)
    for k in range(1, n1):
        s_all = s1[k, 0:1] * s_all + s1[k, 1:2]
        p_all = p_all * s1[k, 0:1]
        p_in = jnp.where(k < me1, p_all, p_in)
        s_in = jnp.where(k < me1, s_all, s_in)
    mine2[0:1, :] = p_all
    mine2[1:2, :] = s_all
    for k in range(1, nz):
        remote(mine2, s2.at[z], xsem.at[4], xsem.at[5], at(dz=k)).start()
    s2[z] = mine2[...]

    @pl.loop(2, 4)
    def _(b):
        gating_block(b)

    for step in range(2, last + 1):
        ring_step(2, step)
    shared_done(2)

    pltpu.make_async_copy(s2.at[pl.ds(0, nz - 1)], s2.at[pl.ds(0, nz - 1)], xsem.at[5]).wait()
    s_plane = jnp.zeros((1, width), F32)
    for k in range(nz - 1):
        s_plane = jnp.where(k < z, s2[k, 0:1] * s_plane + s2[k, 1:2], s_plane)
    carry = p_in * s_plane + s_in
    for g in range(groups):
        lanes = slice(g * LANES, (g + 1) * LANES)
        prod, state = ends[g]
        now = carry[:, lanes]
        for i in range(8):
            cin[g, i:i + 1, :] = now
            now = prod[i:i + 1] * now + state[i:i + 1]

    nt = wb.shape[2]
    tile = wb.shape[3] * wb.shape[4]

    def partial_out(b, emit):
        for i in range(t // chunk):
            r = pl.ds(pl.multiple_of(b * t + i * chunk, chunk), chunk)
            at_chunk = b * (t // chunk) + i
            for g in range(groups):
                lanes = slice(g * LANES, (g + 1) * LANES)
                st = drv[g, r, :] + dec[g, r, :] * cin[g, pl.ds(at_chunk, 1), :]
                mx[i * chunk:(i + 1) * chunk, lanes] = (st * gel[r, lanes]).astype(BF16)

        nt_dims = (((1,), (1,)), ((), ()))

        @pl.loop(0, nz)
        def _(n):
            w0 = wb[2, 0, n].reshape(tile, pw)
            w1 = wb[2, 1, :, n].reshape(tile, pw)
            r = lax.dot_general(mx[:, :pw], w0, nt_dims, preferred_element_type=F32)
            r = r + lax.dot_general(mx[:, pw:], w1, nt_dims, preferred_element_type=F32)
            emit(pl.ds(pl.multiple_of(n * tile, tile), tile), r)

    def emit_to(ref):
        def emit(cols, r):
            ref[:, cols] = r.astype(BF16)
        return emit

    partial_out(far, emit_to(po_far))
    far_a = remote(po_far.at[lo], in_rel.at[0], osend.at[0], orecv.at[0], at(dx=1))
    far_b = remote(po_far.at[hi], in_rel.at[1], osend.at[1], orecv.at[1], at(dx=-1))
    far_a.start()
    far_b.start()
    partial_out(right, emit_to(po_next))
    next_b = remote(po_next.at[hi], in_prev.at[hi], osend.at[2], orecv.at[2], at(dx=1))
    next_b.start()
    partial_out(left, emit_to(po_prev))
    prev_a = remote(po_prev.at[lo], in_next.at[lo], osend.at[3], orecv.at[3], at(dx=-1))
    prev_a.start()

    def emit_own(cols, r):
        outv[:, cols] = r.astype(BF16)

    partial_out(x, emit_own)

    def add_into(ref, base, other):
        @pl.loop(0, half // 16)
        def _(i):
            r = pl.ds(pl.multiple_of(base + i * 16, 16), 16)
            o = pl.ds(pl.multiple_of(i * 16, 16), 16)
            ref[r, :] = (ref[r, :].astype(F32) + other[o, :].astype(F32)).astype(BF16)

    far_a.wait_recv()
    add_into(po_next, 0, in_rel.at[0])
    next_a = remote(po_next.at[lo], in_prev.at[lo], osend.at[4], orecv.at[4], at(dx=1))
    next_a.start()
    far_b.wait_recv()
    add_into(po_prev, half, in_rel.at[1])
    prev_b = remote(po_prev.at[hi], in_next.at[hi], osend.at[5], orecv.at[5], at(dx=-1))
    prev_b.start()

    def finish(base):
        @pl.loop(0, half // 16)
        def _(i):
            r = pl.ds(pl.multiple_of(base + i * 16, 16), 16)
            total = outv[r, :].astype(F32) + in_prev[r, :].astype(F32) + in_next[r, :].astype(F32)
            outv[r, :] = total.astype(BF16)

    next_b.wait_recv()
    prev_a.wait_recv()
    next_a.wait_recv()
    finish(0)
    out_a = pltpu.make_async_copy(outv.at[lo], out.at[lo], lsem.at[0])
    out_a.start()
    prev_b.wait_recv()
    finish(half)
    out_b = pltpu.make_async_copy(outv.at[hi], out.at[hi], lsem.at[1])
    out_b.start()

    for copy in (tok_a_r, tok_b_r, tok_b_l, tok_a_l, rel_a, rel_b, tail_copy, far_a, far_b, next_a, next_b, prev_a, prev_b):
        copy.wait_send()
    for m in range(3):
        pltpu.make_async_copy(dummy, dummy, p1send.at[m]).wait()
        for way in range(2):
            for step in range(last + 1):
                ring_copy(m, way, step).wait_send()
        whole = wb.at[m, c]
        pltpu.make_async_copy(whole, whole, dsend.at[m]).wait()
    pltpu.make_async_copy(s1.at[pl.ds(0, n1 - 1)], s1.at[pl.ds(0, n1 - 1)], xsem.at[2]).wait()
    pltpu.make_async_copy(s2.at[pl.ds(0, nz - 1)], s2.at[pl.ds(0, nz - 1)], xsem.at[4]).wait()
    out_a.wait()
    out_b.wait()


def on_device(
    nz, ny,
    tokens, norm_gain, proj_x, gate_projection, conv_taps, gate_recur, gate_input, decay_param, decay_shift, proj_out,
):
    t, d = tokens.shape
    width = proj_x.shape[1]
    pw = width // 2
    groups = width // LANES
    heads = width // HEAD
    rows = 4 * t
    last = nz // 2
    dma = pltpu.SemaphoreType.DMA
    any_ = pl.BlockSpec(memory_space=pl.ANY)
    vmem = pl.BlockSpec(memory_space=pltpu.VMEM)
    scratch = [
        pltpu.VMEM((4, t, d), BF16),
        pltpu.VMEM((4, t, d), BF16),
        pltpu.VMEM((3, 2, 16, pw), BF16),
        pltpu.VMEM((3, 2, nz, ny, 32, pw), BF16),
        pltpu.VMEM(gate_recur.shape, BF16),
        pltpu.VMEM(gate_input.shape, BF16),
        pltpu.VMEM((rows + 8, width), F32),
        pltpu.VMEM((groups, rows, LANES), F32),
        pltpu.VMEM((groups, rows, LANES), F32),
        pltpu.VMEM((heads, rows, LANES), F32),
        pltpu.VMEM((rows, width), F32),
        pltpu.VMEM((t, width), BF16),
        pltpu.VMEM((8, width), F32),
        pltpu.VMEM((2, width), F32),
        pltpu.VMEM((2 * ny, 2, width), F32),
        pltpu.VMEM((2, width), F32),
        pltpu.VMEM((nz, 2, width), F32),
        pltpu.VMEM((groups, 8, LANES), F32),
        pltpu.VMEM(((ny + nz - 1) * 16, pw), BF16),
        pltpu.VMEM((t, d), BF16),
        pltpu.VMEM((t, d), BF16),
        pltpu.VMEM((t, d), BF16),
        pltpu.VMEM((t, d), BF16),
        pltpu.VMEM((2, t // 2, d), BF16),
        pltpu.VMEM((t, d), BF16),
        pltpu.VMEM((t, d), BF16),
        dma((10,)), dma((2,)), dma((6,)), dma((6,)), dma((3,)), dma((3,)),
        dma((3, 2, last)), dma((3, 2, last)), dma((3,)), dma((3,)), dma((6,)), dma((6,)), dma((6,)),
    ]
    return pl.pallas_call(
        functools.partial(body, nz, ny),
        out_shape=jax.ShapeDtypeStruct((t, d), BF16),
        in_specs=[any_, vmem, any_, any_, vmem, any_, any_, vmem, vmem, any_],
        out_specs=any_,
        scratch_shapes=scratch,
        compiler_params=pltpu.CompilerParams(
            collective_id=0, has_side_effects=True, vmem_limit_bytes=60 * 1024 * 1024
        ),
        name="recurrence",
    )(
        tokens, norm_gain.reshape(1, -1), proj_x, gate_projection, conv_taps, gate_recur, gate_input,
        decay_param.reshape(1, -1), decay_shift, jnp.transpose(proj_out),
    )


def build(mesh, nz, ny):
    split = Mesh(mesh.devices.reshape(nz, ny, 2, mesh.shape["tp"]), ("sp_0", "sp_1", "sp_2", "tp"))
    in_specs = (
        P(SP_TP, None),
        P(),
        P(SP, "tp"),
        P(SP, "tp"),
        P(None, "tp"),
        P("tp", None, None),
        P("tp", None, None),
        P("tp"),
        P("tp", SP),
        P("tp", SP),
    )
    out_specs = P(SP_TP, None)
    return jax.shard_map(
        functools.partial(on_device, nz, ny), mesh=split, in_specs=in_specs, out_specs=out_specs, check_vma=False
    )


def solution(mesh):
    return build(mesh, 8, 8)
```

```python
import functools

import jax
import jax.numpy as jnp
from jax import lax
from jax.experimental import pallas as pl
from jax.experimental.pallas import tpu as pltpu
from jax.sharding import Mesh
from jax.sharding import PartitionSpec as P

HEAD = 256
CONV = 4
SP = ("sp_0", "sp_1", "sp_2")
SP_TP = ("sp_0", "sp_1", "sp_2", "tp")
MESH = pl.DeviceIdType.MESH
F32 = jnp.float32
BF16 = jnp.bfloat16
LANES = 128


def body(
    nz, ny,
    tokens, gain, proj_x, gate_proj, taps, gate_recur, gate_input, decay_param, decay_shift, proj_out,
    out,
    tok, nrm, stage, wb, gr, gi, branch, dec, drv, shiftc, gel, mx, tail,
    mine1, s1, mine2, s2, cin, dummy, outv,
    mixed, relay, acc,
    lsem, gsem, tsend, trecv, p1send, p1recv, rsend, rrecv, dsend, drecv, xsem, osend, orecv, qsend, qrecv,
):
    z, y, c, x = (lax.axis_index(a) for a in SP_TP)
    t = tok.shape[1]
    half = t // 2
    rows = 4 * t
    chunk = rows // 8
    pitch = chunk + 8
    width = 2 * wb.shape[-1]
    groups = width // LANES
    heads = width // HEAD
    pw = width // 2
    nr = wb.shape[2]
    sp_index = (z * ny + y) * 2 + c
    sp_count = nz * ny * 2

    def at(dz=0, dy=0, dc=None, dx=0, core=None):
        cc = c if dc is None else lax.rem(c + dc, 2)
        cc = cc if core is None else core
        return {
            "sp_0": lax.rem(z + dz + nz, nz), "sp_1": lax.rem(y + dy + ny, ny),
            "sp_2": cc, "tp": lax.rem(x + dx + 4, 4),
        }

    def remote(src, dst, send, recv, where):
        return pltpu.make_async_remote_copy(
            src_ref=src, dst_ref=dst, send_sem=send, recv_sem=recv, device_id=where, device_id_type=MESH
        )

    right, left = lax.rem(x + 1, 4), lax.rem(x + 3, 4)
    far = lax.rem(x + 2, 4)

    nsp = lax.rem(sp_index + 1, sp_count)
    psp = lax.rem(sp_index + sp_count - 1, sp_count)

    def of_sp(s):
        return {"sp_0": s // (2 * ny), "sp_1": lax.rem(s // 2, ny), "sp_2": lax.rem(s, 2), "tp": x}

    own_tok = pltpu.make_async_copy(tokens, tok.at[x], lsem.at[0])
    own_tok.start()
    ring = z * (1 - c) + y * c
    cross = y * (1 - c) + z * c
    core_row = pl.multiple_of(c * 16, 16)
    core_col = pl.multiple_of(c * pw, pw)
    stage_loads = []
    for m, src in enumerate((proj_x, gate_proj, proj_out)):
        slot = m if m < 2 else 2 + x
        loads = []
        for p in range(2):
            loads.append(pltpu.make_async_copy(src.at[:, pl.ds(p * pw, pw)], stage.at[slot, p], lsem.at[1 + 3 * m + p]))
        if m < 2:
            loads.append(pltpu.make_async_copy(
                src.at[:, pl.ds(core_col, pw)], wb.at[m, c, ring, cross, pl.ds(core_row, 16)], lsem.at[3 + 3 * m]))
        for load in loads:
            load.start()
        stage_loads.append(loads)
    gate_loads = [
        pltpu.make_async_copy(gate_recur, gr, gsem.at[0]),
        pltpu.make_async_copy(gate_input, gi, gsem.at[1]),
    ]
    for load in gate_loads:
        load.start()

    barrier = pltpu.get_barrier_semaphore()
    peers = [at(dx=1), at(dx=2), at(dx=3)]
    peers += [at(dc=1)]
    peers += [at(dy=k, dc=d) for k in range(1, ny) for d in range(2)]
    peers += [at(dz=k, dc=d) for k in range(1, nz) for d in range(2)]
    peers += [of_sp(nsp), of_sp(psp)]
    for peer in peers:
        pl.semaphore_signal(barrier, inc=1, device_id=peer, device_id_type=MESH)
    pl.semaphore_wait(barrier, len(peers))

    def quarter(k):
        return remote(stage.at[2 + x], stage.at[2 + x], qsend.at[k - 1], qrecv.at[x], at(dx=k))

    def quarters_start():
        for load in stage_loads[2]:
            load.wait()
        for k in range(1, 4):
            quarter(k).start()

    def quarters_done():
        for k in range(1, 4):
            piece_in = stage.at[2 + lax.rem(x + k, 4)]
            pltpu.make_async_copy(piece_in, piece_in, qrecv.at[lax.rem(x + k, 4)]).wait()
        for m in range(2, 6):
            wb[m, c, ring, cross, pl.ds(core_row, 16), :] = stage[m, c]

    def slot(m):
        return m if m < 2 else 2 + lax.rem(x + (0, 3, 1, 2)[m - 2], 4)

    def first_phase(m):
        if m < 2:
            for load in stage_loads[m]:
                load.wait()
        w = slot(m)
        for k in range(1, ny):
            remote(stage.at[w, 0], wb.at[w, 0, z, y, pl.ds(core_row, 16)], p1send.at[m], p1recv.at[m],
                   at(dy=k, core=0)).start()
        for k in range(1, nz):
            remote(stage.at[w, 1], wb.at[w, 1, y, z, pl.ds(core_row, 16)], p1send.at[m], p1recv.at[m],
                   at(dz=k, core=1)).start()
        other = 1 - c
        r2 = z * c + y * (1 - c)
        q2 = y * c + z * (1 - c)
        remote(stage.at[w, other], wb.at[w, other, r2, q2, pl.ds(core_row, 16)], p1send.at[m], p1recv.at[m],
               at(dc=1)).start()

    def ring_at(step):
        return {
            "sp_0": lax.rem(z + (1 - c) * step + nr, nr) * (1 - c) + z * c,
            "sp_1": lax.rem(y + c * step + nr, nr) * c + y * (1 - c),
            "sp_2": c, "tp": x,
        }

    last = nr // 2 - 1
    nq = wb.shape[3]

    def ring_copy(m, way, step, part):
        sign = 1 if way == 0 else -1
        block = lax.rem(ring - sign * step + nr, nr)
        ref = wb.at[slot(m), c, block, pl.ds(part * (nq // 2), nq // 2)]
        return remote(ref, ref, rsend.at[m, way, step, part], rrecv.at[m, way, step, part], ring_at(sign))

    def parts(way, step):
        return (way, 1 - way) if step < last else (way,)

    def share(m, block, part):
        ref = wb.at[slot(m), c, block, pl.ds(part * (nq // 2), nq // 2)]
        remote(ref, ref, dsend.at[m], drecv.at[m], at(dc=1)).start()

    def ring_first(m):
        pltpu.make_async_copy(dummy, dummy, p1recv.at[m]).wait()
        for k in range(2):
            for way in range(2):
                ring_copy(m, way, 0, parts(way, 0)[k]).start()
        for k in range(2):
            share(m, ring, k)

    def ring_step(m, step):
        for k in range(len(parts(0, step))):
            for way in range(2):
                part = parts(way, step)[k]
                ring_copy(m, way, step, part).wait_recv()
                if step < last and part in parts(way, step + 1):
                    ring_copy(m, way, step + 1, part).start()
                sign = 1 if way == 0 else -1
                share(m, lax.rem(ring - sign * (step + 1) + nr, nr), part)

    def shared_done(m):
        whole = wb.at[slot(m), 1 - c]
        pltpu.make_async_copy(whole, whole, drecv.at[m]).wait()

    gain_rows = gain[...].astype(F32)
    gain_row = jnp.concatenate([gain_rows[k:k + 1] for k in range(gain_rows.shape[0])], axis=1)

    def norm_part(b, base, count):
        g = gain_row

        @pl.loop(0, count // 32)
        def _(i):
            r = pl.ds(pl.multiple_of(base + i * 32, 32), 32)
            v = tok[b, r, :].astype(F32)
            s = lax.rsqrt(jnp.mean(v * v, axis=-1, keepdims=True) + 1e-06)
            nrm[b, r, :] = (v * s * g).astype(BF16)

    def weight(m, p):
        if p == 0:
            return wb[m, 0].reshape(-1, pw)
        return jnp.concatenate([wb[m, 1, :, k].reshape(-1, pw) for k in range(nq)], axis=0)

    quarters_start()
    own_tok.wait()
    lo, hi = pl.ds(0, half), pl.ds(half, half)
    tok_a_r = remote(tok.at[x, lo], tok.at[x, lo], tsend.at[0], trecv.at[0], at(dx=1))
    tok_b_r = remote(tok.at[x, hi], tok.at[x, hi], tsend.at[1], trecv.at[1], at(dx=1))
    tok_b_l = remote(tok.at[x, hi], tok.at[x, hi], tsend.at[2], trecv.at[2], at(dx=-1))
    tok_a_l = remote(tok.at[x, lo], tok.at[x, lo], tsend.at[3], trecv.at[3], at(dx=-1))
    rel_a = remote(tok.at[left, lo], tok.at[left, lo], tsend.at[4], trecv.at[4], at(dx=1))
    rel_b = remote(tok.at[right, hi], tok.at[right, hi], tsend.at[5], trecv.at[5], at(dx=-1))
    for copy in (tok_a_r, tok_b_l, tok_b_r, tok_a_l):
        copy.start()

    first_phase(0)
    first_phase(1)
    norm_part(x, 0, t)

    for h in range(heads):
        for k in range(rows // LANES):
            line = decay_shift[h:h + 1, k * LANES:(k + 1) * LANES]
            shiftc[h, k * LANES:(k + 1) * LANES, :] = jnp.transpose(jnp.broadcast_to(line, (LANES, LANES)))
    v = jnp.exp(-decay_param[...])
    rate = v * (1.0 - v * (1 / 2 - v * (1 / 3 - v * (1 / 4 - v * (1 / 5)))))
    rate8 = -8.0 * rate

    queue = [
        (2, 0), (3, 0), (2, 1), (3, 1), (2, 2), (3, 2), (2, 3), (3, 3), (4, 0), (5, 0),
        (2, 4), (3, 4), (4, 1), (5, 1), (4, 2), (5, 2), (4, 3), (5, 3), (4, 4), (5, 4),
    ]
    queue = [(m, k) for m, k in queue if k <= last + 1]

    def pump(count):
        for _ in range(min(count, len(queue))):
            m, k = queue.pop(0)
            if k == 0:
                ring_first(m)
            else:
                ring_step(m, k - 1)

    ring_first(0)
    ring_first(1)
    quarters_done()
    first_phase(2)
    first_phase(3)
    for step in range(last):
        ring_step(0, step)
        ring_step(1, step)
        if step == 0:
            tok_a_r.wait_recv()
            rel_a.start()
            tok_b_l.wait_recv()
            rel_b.start()
        elif step == 1:
            first_phase(4)
            first_phase(5)
            norm_part(left, 0, half)
            norm_part(right, half, half)
    ring_step(0, last)
    ring_step(1, last)
    pump(2)
    tok_b_r.wait_recv()
    tok_a_l.wait_recv()
    norm_part(left, half, half)
    norm_part(right, 0, half)
    shared_done(0)

    def branch_block(b):
        at_row = pl.ds(pl.multiple_of(8 + b * t, 8), t)
        for p in range(2):
            prod = jnp.dot(nrm[b], weight(0, p), preferred_element_type=F32)
            branch[at_row, p * pw:(p + 1) * pw] = prod.astype(BF16).astype(F32)

    @pl.loop(0, 3)
    def _(k):
        branch_block(lax.rem(x + 3 + k, 4))

    pump(2)
    rel_a.wait_recv()
    rel_b.wait_recv()
    norm_part(far, 0, t)
    branch_block(far)

    tail_copy = remote(branch.at[pl.ds(rows, 8)], tail, xsem.at[0], xsem.at[1], of_sp(nsp))
    tail_copy.start()
    for load in gate_loads:
        load.wait()

    tapf = taps[...].astype(F32)

    def gates(i):
        base = pl.multiple_of(i * t, t)
        win = branch[pl.ds(base, t + 8), :]
        acc = jnp.zeros((t, width), F32)
        for k in range(CONV):
            acc = acc + win[5 + k:5 + k + t] * tapf[k:k + 1]
        conv = acc.astype(BF16)
        at_row = pl.ds(base, t)
        for h in range(heads):
            cols = slice(h * HEAD, (h + 1) * HEAD)
            cb = conv[:, cols]
            cf = cb.astype(F32)
            ur = jnp.dot(cb, gr[h], preferred_element_type=F32)
            ui = jnp.dot(cb, gi[h], preferred_element_type=F32)
            recur = 1.0 / (1.0 + jnp.exp(-ur))
            inlet = 1.0 / (1.0 + jnp.exp(-ui))
            sh = shiftc[h, at_row, :]
            log_decay = recur * rate8[:, cols] + jnp.concatenate([sh] * (HEAD // LANES), axis=1)
            decay = jnp.exp(log_decay)
            u = 2.0 * log_decay
            near = u * (1.0 + u * (1 / 2) * (1.0 + u * (1 / 3) * (1.0 + u * (1 / 4) * (1.0 + u * (1 / 5) * (1.0 + u * (1 / 6))))))
            em1 = jnp.where(u > -0.25, near, decay * decay - 1.0)
            drive = jnp.sqrt(-em1) * inlet * cf
            for g in range(HEAD // LANES):
                lanes = slice(g * LANES, (g + 1) * LANES)
                for k in range(t // chunk):
                    part = slice(k * chunk, (k + 1) * chunk)
                    to = pl.ds(pl.multiple_of((i * (t // chunk) + k) * pitch, 8), chunk)
                    dec[h * (HEAD // LANES) + g, to, :] = decay[part, lanes]
                    drv[h * (HEAD // LANES) + g, to, :] = drive[part, lanes]

    @pl.loop(0, 3)
    def _(k):
        gates(3 - k)

    pump(2)

    tail_copy.wait_recv()
    keep = jnp.where(sp_index > 0, 1.0, 0.0).astype(F32)
    branch[0:8, :] = tail[...] * keep
    gates(0)

    def scan_step(j, carried):
        pos = pl.ds(j, 8, stride=pitch)
        new = []
        for g in range(groups):
            prod, state = carried[g]
            a = dec[g, pos, :]
            b = drv[g, pos, :]
            state = a * state + b
            prod = prod * a
            dec[g, pos, :] = prod
            drv[g, pos, :] = state
            new.append((prod, state))
        return tuple(new)

    one, zero = jnp.ones((8, LANES), F32), jnp.zeros((8, LANES), F32)
    ends = lax.fori_loop(0, chunk, scan_step, ((one, zero),) * groups, unroll=4)
    for g in range(groups):
        prod, state = ends[g]
        pr, st = prod[0:1], state[0:1]
        for i in range(1, 8):
            st = prod[i:i + 1] * st + state[i:i + 1]
            pr = pr * prod[i:i + 1]
        mine1[0:1, g * LANES:(g + 1) * LANES] = pr
        mine1[1:2, g * LANES:(g + 1) * LANES] = st

    me1 = y * 2 + c
    n1 = 2 * ny
    firsts = [at(dc=1)] + [at(dy=k, dc=d) for k in range(1, ny) for d in range(2)]
    for peer in firsts:
        remote(mine1, s1.at[me1], xsem.at[2], xsem.at[3], peer).start()
    s1[me1] = mine1[...]

    def gating_block(b):
        for p in range(2):
            cols = slice(p * pw, (p + 1) * pw)
            prod = jnp.dot(nrm[b], weight(1, p), preferred_element_type=F32)
            v = prod.astype(BF16).astype(F32)
            inner = 0.7978845608028654 * (v + 0.044715 * (v * v * v))
            gel[pl.ds(pl.multiple_of(b * t, t), t), cols] = 0.5 * v * (1.0 + jnp.tanh(inner))

    pump(4)
    shared_done(1)

    @pl.loop(0, 2)
    def _(b):
        gating_block(b)

    pump(2)
    pltpu.make_async_copy(s1.at[pl.ds(0, n1 - 1)], s1.at[pl.ds(0, n1 - 1)], xsem.at[3]).wait()
    p_all, s_all = s1[0, 0:1], s1[0, 1:2]
    p_in = jnp.where(me1 > 0, p_all, 1.0)
    s_in = jnp.where(me1 > 0, s_all, 0.0)
    for k in range(1, n1):
        s_all = s1[k, 0:1] * s_all + s1[k, 1:2]
        p_all = p_all * s1[k, 0:1]
        p_in = jnp.where(k < me1, p_all, p_in)
        s_in = jnp.where(k < me1, s_all, s_in)
    mine2[0:1, :] = p_all
    mine2[1:2, :] = s_all
    for k in range(1, nz):
        remote(mine2, s2.at[z], xsem.at[4], xsem.at[5], at(dz=k)).start()
    s2[z] = mine2[...]

    @pl.loop(2, 4)
    def _(b):
        gating_block(b)

    pump(4)
    pltpu.make_async_copy(s2.at[pl.ds(0, nz - 1)], s2.at[pl.ds(0, nz - 1)], xsem.at[5]).wait()
    s_plane = jnp.zeros((1, width), F32)
    for k in range(nz - 1):
        s_plane = jnp.where(k < z, s2[k, 0:1] * s_plane + s2[k, 1:2], s_plane)
    carry = p_in * s_plane + s_in
    for g in range(groups):
        lanes = slice(g * LANES, (g + 1) * LANES)
        prod, state = ends[g]
        now = carry[:, lanes]
        for i in range(8):
            cin[g, i:i + 1, :] = now
            now = prod[i:i + 1] * now + state[i:i + 1]

    def mixed_block(b):
        for g in range(groups):
            parts = []
            lanes = slice(g * LANES, (g + 1) * LANES)
            for i in range(t // chunk):
                at_chunk = b * (t // chunk) + i
                r = pl.ds(pl.multiple_of(at_chunk * pitch, 8), chunk)
                st = drv[g, r, :] + dec[g, r, :] * cin[g, pl.ds(at_chunk, 1), :]
                parts.append(st * gel[pl.ds(pl.multiple_of(at_chunk * chunk, chunk), chunk), lanes])
            mx[b, lanes, :] = jnp.transpose(jnp.concatenate(parts, axis=0)).astype(BF16)

    half_w = width // 2
    wlo, whi = pl.ds(0, half_w), pl.ds(half_w, half_w)
    mixed_block(far)
    far_a = remote(mx.at[far, wlo], relay.at[0], osend.at[0], orecv.at[0], at(dx=1))
    far_b = remote(mx.at[far, whi], relay.at[1], osend.at[1], orecv.at[1], at(dx=-1))
    far_a.start()
    far_b.start()
    mixed_block(right)
    to_right = remote(mx.at[right], mixed.at[x], osend.at[2], orecv.at[2], at(dx=1))
    to_right.start()
    mixed_block(left)
    to_left = remote(mx.at[left], mixed.at[x], osend.at[3], orecv.at[3], at(dx=-1))
    to_left.start()
    mixed_block(x)
    pump(2)
    far_a.wait_recv()
    pass_a = remote(relay.at[0], mixed.at[left, wlo], osend.at[4], orecv.at[4], at(dx=1))
    pass_a.start()
    far_b.wait_recv()
    pass_b = remote(relay.at[1], mixed.at[right, whi], osend.at[5], orecv.at[5], at(dx=-1))
    pass_b.start()
    tile = ny * 32

    def out_tile(m, source, n):
        w0 = wb[slot(m), 0, n].reshape(tile, pw)
        w1 = wb[slot(m), 1, :, n].reshape(tile, pw)
        r = jnp.dot(w0, source[:pw, :], preferred_element_type=F32)
        return r + jnp.dot(w1, source[pw:, :], preferred_element_type=F32)

    shared_done(2)
    @pl.loop(0, nz, unroll=4)
    def _(n):
        acc[n] = out_tile(2, mx[x], n)

    pump(len(queue))
    shared_done(3)
    shared_done(4)
    to_right.wait_recv()
    to_left.wait_recv()

    @pl.loop(0, nz, unroll=4)
    def _(n):
        acc[n] = acc[n] + out_tile(3, mixed[left], n) + out_tile(4, mixed[right], n)

    shared_done(5)
    pass_a.wait_recv()
    pass_b.wait_recv()

    @pl.loop(0, nz, unroll=4)
    def _(n):
        total = acc[n] + out_tile(5, mixed[far], n)
        outv[:, pl.ds(pl.multiple_of(n * tile, tile), tile)] = jnp.transpose(total).astype(BF16)

    out_a = pltpu.make_async_copy(outv, out, lsem.at[0])
    out_a.start()

    for copy in (tok_a_r, tok_b_r, tok_b_l, tok_a_l, rel_a, rel_b, tail_copy, far_a, far_b, to_right, to_left, pass_a, pass_b,
                 quarter(1), quarter(2), quarter(3)):
        copy.wait_send()
    for m in range(6):
        pltpu.make_async_copy(dummy, dummy, p1send.at[m]).wait()
        for way in range(2):
            for step in range(last + 1):
                for part in parts(way, step):
                    ring_copy(m, way, step, part).wait_send()
        whole = wb.at[slot(m), c]
        pltpu.make_async_copy(whole, whole, dsend.at[m]).wait()
    pltpu.make_async_copy(s1.at[pl.ds(0, n1 - 1)], s1.at[pl.ds(0, n1 - 1)], xsem.at[2]).wait()
    pltpu.make_async_copy(s2.at[pl.ds(0, nz - 1)], s2.at[pl.ds(0, nz - 1)], xsem.at[4]).wait()
    out_a.wait()


def on_device(
    nz, ny,
    tokens, norm_gain, proj_x, gate_projection, conv_taps, gate_recur, gate_input, decay_param, decay_shift, proj_out,
):
    t, d = tokens.shape
    width = proj_x.shape[1]
    pw = width // 2
    groups = width // LANES
    heads = width // HEAD
    rows = 4 * t
    last = nz // 2
    dma = pltpu.SemaphoreType.DMA
    any_ = pl.BlockSpec(memory_space=pl.ANY)
    vmem = pl.BlockSpec(memory_space=pltpu.VMEM)
    scratch = [
        pltpu.VMEM((4, t, d), BF16),
        pltpu.VMEM((4, t, d), BF16),
        pltpu.VMEM((6, 2, 16, pw), BF16),
        pltpu.VMEM((6, 2, nz, ny, 32, pw), BF16),
        pltpu.VMEM(gate_recur.shape, BF16),
        pltpu.VMEM(gate_input.shape, BF16),
        pltpu.VMEM((rows + 8, width), F32),
        pltpu.VMEM((groups, rows + 64, LANES), F32),
        pltpu.VMEM((groups, rows + 64, LANES), F32),
        pltpu.VMEM((heads, rows, LANES), F32),
        pltpu.VMEM((rows, width), F32),
        pltpu.VMEM((4, width, t), BF16),
        pltpu.VMEM((8, width), F32),
        pltpu.VMEM((2, width), F32),
        pltpu.VMEM((2 * ny, 2, width), F32),
        pltpu.VMEM((2, width), F32),
        pltpu.VMEM((nz, 2, width), F32),
        pltpu.VMEM((groups, 8, LANES), F32),
        pltpu.VMEM(((ny + nz - 1) * 16, pw), BF16),
        pltpu.VMEM((t, d), BF16),
        pltpu.VMEM((4, width, t), BF16),
        pltpu.VMEM((2, width // 2, t), BF16),
        pltpu.VMEM((nz, ny * 32, t), F32),
        dma((10,)), dma((2,)), dma((6,)), dma((6,)), dma((6,)), dma((6,)),
        dma((6, 2, last, 2)), dma((6, 2, last, 2)), dma((6,)), dma((6,)), dma((6,)), dma((6,)), dma((6,)), dma((3,)), dma((4,)),
    ]
    return pl.pallas_call(
        functools.partial(body, nz, ny),
        out_shape=jax.ShapeDtypeStruct((t, d), BF16),
        in_specs=[any_, vmem, any_, any_, vmem, any_, any_, vmem, vmem, any_],
        out_specs=any_,
        scratch_shapes=scratch,
        compiler_params=pltpu.CompilerParams(
            collective_id=0, has_side_effects=True, vmem_limit_bytes=60 * 1024 * 1024
        ),
        name="recurrence",
    )(
        tokens, norm_gain.reshape(-1, LANES), proj_x, gate_projection, conv_taps, gate_recur, gate_input,
        decay_param.reshape(1, -1), decay_shift, jnp.transpose(proj_out),
    )


def build(mesh, nz, ny):
    split = Mesh(mesh.devices.reshape(nz, ny, 2, mesh.shape["tp"]), ("sp_0", "sp_1", "sp_2", "tp"))
    in_specs = (
        P(SP_TP, None),
        P(),
        P(SP, "tp"),
        P(SP, "tp"),
        P(None, "tp"),
        P("tp", None, None),
        P("tp", None, None),
        P("tp"),
        P("tp", SP),
        P("tp", SP),
    )
    out_specs = P(SP_TP, None)
    return jax.shard_map(
        functools.partial(on_device, nz, ny), mesh=split, in_specs=in_specs, out_specs=out_specs, check_vma=False
    )


def solution(mesh):
    return build(mesh, 8, 8)
```

```python
import functools

import jax
import jax.numpy as jnp
from jax import lax
from jax.experimental import pallas as pl
from jax.experimental.pallas import tpu as pltpu
from jax.sharding import Mesh
from jax.sharding import PartitionSpec as P

HEAD = 256
CONV = 4
SP = ("sp_0", "sp_1", "sp_2")
SP_TP = ("sp_0", "sp_1", "sp_2", "tp")
MESH = pl.DeviceIdType.MESH
F32 = jnp.float32
BF16 = jnp.bfloat16
HALVED = (4, 5)
PLAN = {
    "start": ("P1",),
    "r0": ("R10", "Q", "P4", "P5",),
    "s0": ("R11",),
    "s1": ("R12", "P2", "P3",),
    "s2": ("R13", "R40", "R50",),
    "last": ("R14", "R41", "R51", "R20", "R30",),
    "far": ("R42", "R52",),
    "g2": ("R21", "R31",),
    "scan": ("R43", "R53",),
    "w1": ("R22", "R32",),
    "f1": ("R44", "R54",),
    "w2": ("R23", "R33",),
    "mix": ("R24", "R34", "S4", "S5",),
}
GATING = 2
LANES = 128


def body(
    nz, ny,
    tokens, gain, proj_x, gate_proj, taps, gate_recur, gate_input, decay_param, decay_shift, proj_out,
    out,
    tok, nrm, stage, wb, gr, gi, branch, dec, drv, shiftc, gel, mx, tail,
    mine1, s1, mine2, s2, cin, dummy, outv,
    mixed, relay, acc,
    lsem, gsem, tsend, trecv, p1send, p1recv, rsend, rrecv, dsend, drecv, xsem, osend, orecv, qsend, qrecv, swapsend, swaprecv,
):
    z, y, c, x = (lax.axis_index(a) for a in SP_TP)
    t = tok.shape[1]
    half = t // 2
    rows = 4 * t
    chunk = rows // 8
    pitch = chunk + 8
    width = 2 * wb.shape[-1]
    groups = width // LANES
    heads = width // HEAD
    pw = width // 2
    nr = wb.shape[2]
    sp_index = (z * ny + y) * 2 + c
    sp_count = nz * ny * 2

    def at(dz=0, dy=0, dc=None, dx=0, core=None):
        cc = c if dc is None else lax.rem(c + dc, 2)
        cc = cc if core is None else core
        return {
            "sp_0": lax.rem(z + dz + nz, nz), "sp_1": lax.rem(y + dy + ny, ny),
            "sp_2": cc, "tp": lax.rem(x + dx + 4, 4),
        }

    def remote(src, dst, send, recv, where):
        return pltpu.make_async_remote_copy(
            src_ref=src, dst_ref=dst, send_sem=send, recv_sem=recv, device_id=where, device_id_type=MESH
        )

    right, left = lax.rem(x + 1, 4), lax.rem(x + 3, 4)
    far = lax.rem(x + 2, 4)

    nsp = lax.rem(sp_index + 1, sp_count)
    psp = lax.rem(sp_index + sp_count - 1, sp_count)

    def of_sp(s):
        return {"sp_0": s // (2 * ny), "sp_1": lax.rem(s // 2, ny), "sp_2": lax.rem(s, 2), "tp": x}

    own_tok = pltpu.make_async_copy(tokens, tok.at[x], lsem.at[0])
    own_tok.start()
    ring = z * (1 - c) + y * c
    cross = y * (1 - c) + z * c
    core_row = pl.multiple_of(c * 16, 16)
    core_col = pl.multiple_of(c * pw, pw)
    stage_loads = []
    for m, src in enumerate((proj_x, gate_proj, proj_out)):
        slot = m if m < 2 else 2 + x
        loads = []
        for p in range(2):
            loads.append(pltpu.make_async_copy(src.at[:, pl.ds(p * pw, pw)], stage.at[slot, p], lsem.at[1 + 3 * m + p]))
        if m < 2:
            loads.append(pltpu.make_async_copy(
                src.at[:, pl.ds(core_col, pw)], wb.at[m, c, ring, cross, pl.ds(core_row, 16)], lsem.at[3 + 3 * m]))
        for load in loads:
            load.start()
        stage_loads.append(loads)
    gate_loads = [
        pltpu.make_async_copy(gate_recur, gr, gsem.at[0]),
        pltpu.make_async_copy(gate_input, gi, gsem.at[1]),
    ]
    for load in gate_loads:
        load.start()

    barrier = pltpu.get_barrier_semaphore()
    peers = [at(dx=1), at(dx=2), at(dx=3)]
    peers += [at(dc=1)]
    peers += [at(dy=k, dc=d) for k in range(1, ny) for d in range(2)]
    peers += [at(dz=k, dc=d) for k in range(1, nz) for d in range(2)]
    peers += [of_sp(nsp), of_sp(psp)]
    for peer in peers:
        pl.semaphore_signal(barrier, inc=1, device_id=peer, device_id_type=MESH)
    pl.semaphore_wait(barrier, len(peers))

    def quarter(k):
        return remote(stage.at[2 + x], stage.at[2 + x], qsend.at[k - 1], qrecv.at[x], at(dx=k))

    def quarters_start():
        for load in stage_loads[2]:
            load.wait()
        for k in range(1, 4):
            quarter(k).start()

    def quarters_done():
        for k in range(1, 4):
            piece_in = stage.at[2 + lax.rem(x + k, 4)]
            pltpu.make_async_copy(piece_in, piece_in, qrecv.at[lax.rem(x + k, 4)]).wait()
        for m in range(2, 6):
            def put(m=m):
                wb[m, c, ring, cross, pl.ds(core_row, 16), :] = stage[m, c]
            given(m, cross, put)

    nq = wb.shape[3]
    hq = nq // 2
    last = nr // 2 - 1
    other = 1 - c
    away_r = z * c + y * (1 - c)
    away_q = y * c + z * (1 - c)

    def mine(m):
        return lax.rem(x + m, 2)

    def pieces(m):
        sends = [
            (y, [(stage.at[m, 0], wb.at[m, 0, z, y, pl.ds(core_row, 16)], at(dy=k, core=0)) for k in range(1, ny)]),
            (z, [(stage.at[m, 1], wb.at[m, 1, y, z, pl.ds(core_row, 16)], at(dz=k, core=1)) for k in range(1, nz)]),
            (away_q, [(stage.at[m, other], wb.at[m, other, away_r, away_q, pl.ds(core_row, 16)], at(dc=1))]),
        ]
        return sends

    def given(m, q, act):
        if m in HALVED:
            pl.when(q // hq == mine(m))(act)
        else:
            act()

    def first_phase(m):
        if m < 2:
            for load in stage_loads[m]:
                load.wait()
        for k, (q, sends) in enumerate(pieces(m)):
            def act(k=k, sends=sends):
                for src, dst, where in sends:
                    remote(src, dst, p1send.at[m, k], p1recv.at[m], where).start()
            given(m, q, act)

    def wait_rows(sem, count):
        ref = dummy.at[pl.ds(0, 16 * count)]
        pltpu.make_async_copy(ref, ref, sem).wait()

    def first_phase_done(m):
        if m in HALVED:
            own = cross // hq == mine(m)
            pl.when(own)(lambda: wait_rows(p1recv.at[m], nq - 1))
            pl.when(jnp.logical_not(own))(lambda: wait_rows(p1recv.at[m], nq))
        else:
            wait_rows(p1recv.at[m], 2 * nq - 1)

    def first_phase_sent(m):
        for k, (q, sends) in enumerate(pieces(m)):
            given(m, q, lambda k=k, sends=sends: wait_rows(p1send.at[m, k], len(sends)))

    def ring_at(step):
        return {
            "sp_0": lax.rem(z + (1 - c) * step + nr, nr) * (1 - c) + z * c,
            "sp_1": lax.rem(y + c * step + nr, nr) * c + y * (1 - c),
            "sp_2": c, "tp": x,
        }

    def half_block(m, block, part):
        return wb.at[m, c, block, pl.ds(part * hq, hq)]

    def ring_block(way, step):
        return lax.rem(ring - (1 if way == 0 else -1) * step + nr, nr)

    def ring_copy(m, way, step, part):
        ref = half_block(m, ring_block(way, step), mine(m) if m in HALVED else part)
        return remote(ref, ref, rsend.at[m, way, step, part], rrecv.at[m, way, step, part],
                      ring_at(1 if way == 0 else -1))

    def parts(m, way, step):
        if m in HALVED:
            return (0,)
        return (way, 1 - way) if step < last else (way,)

    def turn(m, way, step, act):
        if m in HALVED and step == last:
            pl.when(mine(m) == way)(act)
        else:
            act()

    def share(m, block, part):
        ref = half_block(m, block, mine(m) if m in HALVED else part)
        remote(ref, ref, dsend.at[m], drecv.at[m], at(dc=1)).start()
        if m in HALVED:
            remote(ref, ref, swapsend.at[m], swaprecv.at[m], at(dx=1 - 2 * (block // (nr // 2)))).start()

    def ring_first(m):
        first_phase_done(m)
        for k in range(len(parts(m, 0, 0))):
            for way in range(2):
                ring_copy(m, way, 0, parts(m, way, 0)[k]).start()
        for part in sorted(parts(m, 0, 0)):
            share(m, ring, part)

    def ring_step(m, step):
        for k in range(len(parts(m, 0, step))):
            for way in range(2):
                part = parts(m, way, step)[k]

                def act(way=way, part=part):
                    ring_copy(m, way, step, part).wait_recv()
                    if step < last and part in parts(m, way, step + 1):
                        turn(m, way, step + 1, lambda: ring_copy(m, way, step + 1, part).start())
                    share(m, ring_block(way, step + 1), part)

                turn(m, way, step, act)

    def ring_sent(m):
        for way in range(2):
            for step in range(last + 1):
                for part in parts(m, way, step):
                    turn(m, way, step, lambda: ring_copy(m, way, step, part).wait_send())
        if m in HALVED:
            ref = wb.at[m, c, :, pl.ds(0, hq)]
            pltpu.make_async_copy(ref, ref, swapsend.at[m]).wait()
        whole = wb.at[m, c]
        pltpu.make_async_copy(whole, whole, dsend.at[m]).wait()

    def swapped(m):
        if m in HALVED:
            ref = wb.at[m, c, :, pl.ds((1 - mine(m)) * hq, hq)]
            pltpu.make_async_copy(ref, ref, swaprecv.at[m]).wait()
            remote(ref, ref, dsend.at[m], drecv.at[m], at(dc=1)).start()

    def shared_done(m):
        whole = wb.at[m, 1 - c]
        pltpu.make_async_copy(whole, whole, drecv.at[m]).wait()

    gain_rows = gain[...].astype(F32)
    gain_row = jnp.concatenate([gain_rows[k:k + 1] for k in range(gain_rows.shape[0])], axis=1)

    def norm_part(b, base, count):
        g = gain_row

        @pl.loop(0, count // 32)
        def _(i):
            r = pl.ds(pl.multiple_of(base + i * 32, 32), 32)
            v = tok[b, r, :].astype(F32)
            s = lax.rsqrt(jnp.mean(v * v, axis=-1, keepdims=True) + 1e-06)
            nrm[b, r, :] = (v * s * g).astype(BF16)

    def weight(m, p):
        if p == 0:
            return wb[m, 0].reshape(-1, pw)
        return jnp.concatenate([wb[m, 1, :, k].reshape(-1, pw) for k in range(nq)], axis=0)

    def carry_on(place):
        for op in PLAN.get(place, ()):
            m = int(op[1:2] or 0)
            if op[0] == "P":
                first_phase(m)
            elif op[0] == "Q":
                quarters_done()
            elif op[0] == "S":
                swapped(m)
            elif op[2] == "0":
                ring_first(m)
            else:
                ring_step(m, int(op[2]) - 1)

    quarters_start()
    own_tok.wait()
    lo, hi = pl.ds(0, half), pl.ds(half, half)
    tok_a_r = remote(tok.at[x, lo], tok.at[x, lo], tsend.at[0], trecv.at[0], at(dx=1))
    tok_b_r = remote(tok.at[x, hi], tok.at[x, hi], tsend.at[1], trecv.at[1], at(dx=1))
    tok_b_l = remote(tok.at[x, hi], tok.at[x, hi], tsend.at[2], trecv.at[2], at(dx=-1))
    tok_a_l = remote(tok.at[x, lo], tok.at[x, lo], tsend.at[3], trecv.at[3], at(dx=-1))
    rel_a = remote(tok.at[left, lo], tok.at[left, lo], tsend.at[4], trecv.at[4], at(dx=1))
    rel_b = remote(tok.at[right, hi], tok.at[right, hi], tsend.at[5], trecv.at[5], at(dx=-1))
    for copy in (tok_a_r, tok_b_l, tok_b_r, tok_a_l):
        copy.start()

    first_phase(0)
    carry_on("start")
    norm_part(x, 0, t)

    for h in range(heads):
        for k in range(rows // LANES):
            line = decay_shift[h:h + 1, k * LANES:(k + 1) * LANES]
            shiftc[h, k * LANES:(k + 1) * LANES, :] = jnp.transpose(jnp.broadcast_to(line, (LANES, LANES)))
    v = jnp.exp(-decay_param[...])
    rate = v * (1.0 - v * (1 / 2 - v * (1 / 3 - v * (1 / 4 - v * (1 / 5)))))
    rate8 = -8.0 * rate

    ring_first(0)
    carry_on("r0")
    ring_step(0, 0)
    tok_a_r.wait_recv()
    rel_a.start()
    tok_b_l.wait_recv()
    rel_b.start()
    carry_on("s0")
    ring_step(0, 1)
    carry_on("s1")
    norm_part(left, 0, half)
    norm_part(right, half, half)
    ring_step(0, 2)
    carry_on("s2")
    tok_b_r.wait_recv()
    tok_a_l.wait_recv()
    norm_part(left, half, half)
    norm_part(right, 0, half)
    rel_a.wait_recv()
    rel_b.wait_recv()
    norm_part(far, 0, t)
    ring_step(0, last)
    carry_on("last")
    shared_done(0)

    def branch_block(b):
        at_row = pl.ds(pl.multiple_of(8 + b * t, 8), t)
        for p in range(2):
            prod = jnp.dot(nrm[b], weight(0, p), preferred_element_type=F32)
            branch[at_row, p * pw:(p + 1) * pw] = prod.astype(BF16).astype(F32)

    @pl.loop(0, 4)
    def _(b):
        branch_block(b)

    carry_on("branch")

    tail_copy = remote(branch.at[pl.ds(rows, 8)], tail, xsem.at[0], xsem.at[1], of_sp(nsp))
    tail_copy.start()
    carry_on("far")
    for load in gate_loads:
        load.wait()

    tapf = taps[...].astype(F32)

    def gates(i):
        base = pl.multiple_of(i * t, t)
        win = branch[pl.ds(base, t + 8), :]
        acc = jnp.zeros((t, width), F32)
        for k in range(CONV):
            acc = acc + win[5 + k:5 + k + t] * tapf[k:k + 1]
        conv = acc.astype(BF16)
        at_row = pl.ds(base, t)
        for h in range(heads):
            cols = slice(h * HEAD, (h + 1) * HEAD)
            cb = conv[:, cols]
            cf = cb.astype(F32)
            ur = jnp.dot(cb, gr[h], preferred_element_type=F32)
            ui = jnp.dot(cb, gi[h], preferred_element_type=F32)
            recur = 1.0 / (1.0 + jnp.exp(-ur))
            inlet = 1.0 / (1.0 + jnp.exp(-ui))
            sh = shiftc[h, at_row, :]
            log_decay = recur * rate8[:, cols] + jnp.concatenate([sh] * (HEAD // LANES), axis=1)
            decay = jnp.exp(log_decay)
            u = 2.0 * log_decay
            near = u * (1.0 + u * (1 / 2) * (1.0 + u * (1 / 3) * (1.0 + u * (1 / 4) * (1.0 + u * (1 / 5) * (1.0 + u * (1 / 6))))))
            em1 = jnp.where(u > -0.25, near, decay * decay - 1.0)
            drive = jnp.sqrt(-em1) * inlet * cf
            for g in range(HEAD // LANES):
                lanes = slice(g * LANES, (g + 1) * LANES)
                for k in range(t // chunk):
                    part = slice(k * chunk, (k + 1) * chunk)
                    to = pl.ds(pl.multiple_of((i * (t // chunk) + k) * pitch, 8), chunk)
                    dec[h * (HEAD // LANES) + g, to, :] = decay[part, lanes]
                    drv[h * (HEAD // LANES) + g, to, :] = drive[part, lanes]

    gates(3)
    carry_on("g3")
    gates(2)
    carry_on("g2")
    gates(1)
    carry_on("g1")

    tail_copy.wait_recv()
    keep = jnp.where(sp_index > 0, 1.0, 0.0).astype(F32)
    branch[0:8, :] = tail[...] * keep
    gates(0)

    def scan_step(j, carried):
        pos = pl.ds(j, 8, stride=pitch)
        new = []
        for g in range(groups):
            prod, state = carried[g]
            a = dec[g, pos, :]
            b = drv[g, pos, :]
            state = a * state + b
            prod = prod * a
            dec[g, pos, :] = prod
            drv[g, pos, :] = state
            new.append((prod, state))
        return tuple(new)

    one, zero = jnp.ones((8, LANES), F32), jnp.zeros((8, LANES), F32)
    ends = lax.fori_loop(0, chunk, scan_step, ((one, zero),) * groups, unroll=4)
    for g in range(groups):
        prod, state = ends[g]
        pr, st = prod[0:1], state[0:1]
        for i in range(1, 8):
            st = prod[i:i + 1] * st + state[i:i + 1]
            pr = pr * prod[i:i + 1]
        mine1[0:1, g * LANES:(g + 1) * LANES] = pr
        mine1[1:2, g * LANES:(g + 1) * LANES] = st

    me1 = y * 2 + c
    n1 = 2 * ny
    firsts = [at(dc=1)] + [at(dy=k, dc=d) for k in range(1, ny) for d in range(2)]
    for peer in firsts:
        remote(mine1, s1.at[me1], xsem.at[2], xsem.at[3], peer).start()
    s1[me1] = mine1[...]

    def gating_block(b):
        for p in range(2):
            cols = slice(p * pw, (p + 1) * pw)
            prod = jnp.dot(nrm[b], weight(1, p), preferred_element_type=F32)
            v = prod.astype(BF16).astype(F32)
            inner = 0.7978845608028654 * (v + 0.044715 * (v * v * v))
            gel[pl.ds(pl.multiple_of(b * t, t), t), cols] = 0.5 * v * (1.0 + jnp.tanh(inner))

    def gating(first, end):
        if end > first:
            @pl.loop(first, end)
            def _(b):
                gating_block(b)

    carry_on("scan")
    if GATING:
        shared_done(1)
        gating(0, GATING)
    carry_on("w1")
    pltpu.make_async_copy(s1.at[pl.ds(0, n1 - 1)], s1.at[pl.ds(0, n1 - 1)], xsem.at[3]).wait()
    p_all, s_all = s1[0, 0:1], s1[0, 1:2]
    p_in = jnp.where(me1 > 0, p_all, 1.0)
    s_in = jnp.where(me1 > 0, s_all, 0.0)
    for k in range(1, n1):
        s_all = s1[k, 0:1] * s_all + s1[k, 1:2]
        p_all = p_all * s1[k, 0:1]
        p_in = jnp.where(k < me1, p_all, p_in)
        s_in = jnp.where(k < me1, s_all, s_in)
    mine2[0:1, :] = p_all
    mine2[1:2, :] = s_all
    for k in range(1, nz):
        remote(mine2, s2.at[z], xsem.at[4], xsem.at[5], at(dz=k)).start()
    s2[z] = mine2[...]

    carry_on("f1")
    if not GATING:
        shared_done(1)
    gating(GATING, 4)
    carry_on("w2")
    pltpu.make_async_copy(s2.at[pl.ds(0, nz - 1)], s2.at[pl.ds(0, nz - 1)], xsem.at[5]).wait()
    s_plane = jnp.zeros((1, width), F32)
    for k in range(nz - 1):
        s_plane = jnp.where(k < z, s2[k, 0:1] * s_plane + s2[k, 1:2], s_plane)
    carry = p_in * s_plane + s_in
    for g in range(groups):
        lanes = slice(g * LANES, (g + 1) * LANES)
        prod, state = ends[g]
        now = carry[:, lanes]
        for i in range(8):
            cin[g, i:i + 1, :] = now
            now = prod[i:i + 1] * now + state[i:i + 1]

    def mixed_block(b):
        for g in range(groups):
            parts = []
            lanes = slice(g * LANES, (g + 1) * LANES)
            for i in range(t // chunk):
                at_chunk = b * (t // chunk) + i
                r = pl.ds(pl.multiple_of(at_chunk * pitch, 8), chunk)
                st = drv[g, r, :] + dec[g, r, :] * cin[g, pl.ds(at_chunk, 1), :]
                parts.append(st * gel[pl.ds(pl.multiple_of(at_chunk * chunk, chunk), chunk), lanes])
            mx[b, lanes, :] = jnp.transpose(jnp.concatenate(parts, axis=0)).astype(BF16)

    half_w = width // 2
    wlo, whi = pl.ds(0, half_w), pl.ds(half_w, half_w)
    mixed_block(far)
    far_a = remote(mx.at[far, wlo], relay.at[0], osend.at[0], orecv.at[0], at(dx=1))
    far_b = remote(mx.at[far, whi], relay.at[1], osend.at[1], orecv.at[1], at(dx=-1))
    far_a.start()
    far_b.start()
    mixed_block(right)
    to_right = remote(mx.at[right], mixed.at[x], osend.at[2], orecv.at[2], at(dx=1))
    to_right.start()
    mixed_block(left)
    to_left = remote(mx.at[left], mixed.at[x], osend.at[3], orecv.at[3], at(dx=-1))
    to_left.start()
    mixed_block(x)
    carry_on("mix")
    far_a.wait_recv()
    pass_a = remote(relay.at[0], mixed.at[left, wlo], osend.at[4], orecv.at[4], at(dx=1))
    pass_a.start()
    far_b.wait_recv()
    pass_b = remote(relay.at[1], mixed.at[right, whi], osend.at[5], orecv.at[5], at(dx=-1))
    pass_b.start()
    carry_on("rel")

    tile = ny * 32

    def out_tile(q, source, n):
        w0 = wb[2 + q, 0, n].reshape(tile, pw)
        w1 = wb[2 + q, 1, :, n].reshape(tile, pw)
        r = jnp.dot(w0, source[:pw, :], preferred_element_type=F32)
        return r + jnp.dot(w1, source[pw:, :], preferred_element_type=F32)

    for m in range(2, 6):
        shared_done(m)
    @pl.loop(0, nz, unroll=4)
    def _(n):
        acc[n] = out_tile(x, mx[x], n)

    to_right.wait_recv()
    to_left.wait_recv()

    @pl.loop(0, nz, unroll=4)
    def _(n):
        acc[n] = acc[n] + out_tile(left, mixed[left], n) + out_tile(right, mixed[right], n)

    pass_a.wait_recv()
    pass_b.wait_recv()
    leave = []
    for k in range(2):
        @pl.loop(k * (nz // 2), (k + 1) * (nz // 2), unroll=nz // 2)
        def _(n):
            total = acc[n] + out_tile(far, mixed[far], n)
            outv[:, pl.ds(pl.multiple_of(n * tile, tile), tile)] = jnp.transpose(total).astype(BF16)

        side = pl.ds(k * (nz // 2) * tile, (nz // 2) * tile)
        leave.append(pltpu.make_async_copy(outv.at[:, side], out.at[:, side], lsem.at[k]))
        leave[k].start()

    for copy in (tok_a_r, tok_b_r, tok_b_l, tok_a_l, rel_a, rel_b, tail_copy, far_a, far_b, to_right, to_left, pass_a, pass_b,
                 quarter(1), quarter(2), quarter(3)):
        copy.wait_send()
    for m in range(6):
        first_phase_sent(m)
        ring_sent(m)
    pltpu.make_async_copy(s1.at[pl.ds(0, n1 - 1)], s1.at[pl.ds(0, n1 - 1)], xsem.at[2]).wait()
    pltpu.make_async_copy(s2.at[pl.ds(0, nz - 1)], s2.at[pl.ds(0, nz - 1)], xsem.at[4]).wait()
    for copy in leave:
        copy.wait()


def on_device(
    nz, ny,
    tokens, norm_gain, proj_x, gate_projection, conv_taps, gate_recur, gate_input, decay_param, decay_shift, proj_out,
):
    t, d = tokens.shape
    width = proj_x.shape[1]
    pw = width // 2
    groups = width // LANES
    heads = width // HEAD
    rows = 4 * t
    last = nz // 2
    dma = pltpu.SemaphoreType.DMA
    any_ = pl.BlockSpec(memory_space=pl.ANY)
    vmem = pl.BlockSpec(memory_space=pltpu.VMEM)
    scratch = [
        pltpu.VMEM((4, t, d), BF16),
        pltpu.VMEM((4, t, d), BF16),
        pltpu.VMEM((6, 2, 16, pw), BF16),
        pltpu.VMEM((6, 2, nz, ny, 32, pw), BF16),
        pltpu.VMEM(gate_recur.shape, BF16),
        pltpu.VMEM(gate_input.shape, BF16),
        pltpu.VMEM((rows + 8, width), F32),
        pltpu.VMEM((groups, rows + 64, LANES), F32),
        pltpu.VMEM((groups, rows + 64, LANES), F32),
        pltpu.VMEM((heads, rows, LANES), F32),
        pltpu.VMEM((rows, width), F32),
        pltpu.VMEM((4, width, t), BF16),
        pltpu.VMEM((8, width), F32),
        pltpu.VMEM((2, width), F32),
        pltpu.VMEM((2 * ny, 2, width), F32),
        pltpu.VMEM((2, width), F32),
        pltpu.VMEM((nz, 2, width), F32),
        pltpu.VMEM((groups, 8, LANES), F32),
        pltpu.VMEM(((ny + nz - 1) * 16, pw), BF16),
        pltpu.VMEM((t, d), BF16),
        pltpu.VMEM((4, width, t), BF16),
        pltpu.VMEM((2, width // 2, t), BF16),
        pltpu.VMEM((nz, ny * 32, t), F32),
        dma((10,)), dma((2,)), dma((6,)), dma((6,)), dma((6, 3)), dma((6,)),
        dma((6, 2, last, 2)), dma((6, 2, last, 2)), dma((6,)), dma((6,)), dma((6,)), dma((6,)), dma((6,)), dma((3,)), dma((4,)),
        dma((6,)), dma((6,)),
    ]
    return pl.pallas_call(
        functools.partial(body, nz, ny),
        out_shape=jax.ShapeDtypeStruct((t, d), BF16),
        in_specs=[any_, vmem, any_, any_, vmem, any_, any_, vmem, vmem, any_],
        out_specs=any_,
        scratch_shapes=scratch,
        compiler_params=pltpu.CompilerParams(
            collective_id=0, has_side_effects=True, vmem_limit_bytes=60 * 1024 * 1024
        ),
        name="recurrence",
    )(
        tokens, norm_gain.reshape(-1, LANES), proj_x, gate_projection, conv_taps, gate_recur, gate_input,
        decay_param.reshape(1, -1), decay_shift, jnp.transpose(proj_out),
    )


def build(mesh, nz, ny):
    split = Mesh(mesh.devices.reshape(nz, ny, 2, mesh.shape["tp"]), ("sp_0", "sp_1", "sp_2", "tp"))
    in_specs = (
        P(SP_TP, None),
        P(),
        P(SP, "tp"),
        P(SP, "tp"),
        P(None, "tp"),
        P("tp", None, None),
        P("tp", None, None),
        P("tp"),
        P("tp", SP),
        P("tp", SP),
    )
    out_specs = P(SP_TP, None)
    return jax.shard_map(
        functools.partial(on_device, nz, ny), mesh=split, in_specs=in_specs, out_specs=out_specs, check_vma=False
    )


def solution(mesh):
    return build(mesh, 8, 8)
```

```python
import functools

import jax
import jax.numpy as jnp
from jax import lax
from jax.experimental import pallas as pl
from jax.experimental.pallas import tpu as pltpu
from jax.sharding import Mesh
from jax.sharding import PartitionSpec as P

HEAD = 256
CONV = 4
SP = ("sp_0", "sp_1", "sp_2")
SP_TP = ("sp_0", "sp_1", "sp_2", "tp")
MESH = pl.DeviceIdType.MESH
F32 = jnp.float32
BF16 = jnp.bfloat16
HALVED = (4, 5)
PLAN = {
    "start": ("P1",),
    "r0": ("R10", "Q", "P4", "P5",),
    "s0": ("R11",),
    "s1": ("R12", "P2", "P3",),
    "s2": ("R13", "R40", "R50",),
    "last": ("R14", "R41", "R51", "R20", "R30",),
    "far": ("R42", "R52",),
    "g2": ("R21", "R31",),
    "scan": ("R43", "R53",),
    "w1": ("R22", "R32",),
    "f1": ("R44", "R54",),
    "w2": ("R23", "R33",),
    "mix": ("R24", "R34", "S4", "S5",),
}
GATING = 2
LANES = 128


def body(
    nz, ny,
    tokens, gain_in, proj_x, gate_proj, taps_in, gate_recur, gate_input, param_in, shift_in, proj_out,
    out,
    tok, nrm, stage, wb, gr, gi, branch, dec, drv, shiftc, gel, mx, tail,
    mine1, s1, mine2, s2, cin, dummy, outv,
    mixed, relay, acc,
    gain, taps, decay_param, decay_shift,
    lsem, gsem, tsend, trecv, p1send, p1recv, rsend, rrecv, dsend, drecv, xsem, osend, orecv, qsend, qrecv, swapsend, swaprecv,
):
    z, y, c, x = (lax.axis_index(a) for a in SP_TP)
    t = tok.shape[1]
    half = t // 2
    rows = 4 * t
    chunk = rows // 8
    pitch = chunk + 8
    width = 2 * wb.shape[-1]
    groups = width // LANES
    heads = width // HEAD
    pw = width // 2
    nr = wb.shape[2]
    sp_index = (z * ny + y) * 2 + c
    sp_count = nz * ny * 2

    def at(dz=0, dy=0, dc=None, dx=0, core=None):
        cc = c if dc is None else lax.rem(c + dc, 2)
        cc = cc if core is None else core
        return {
            "sp_0": lax.rem(z + dz + nz, nz), "sp_1": lax.rem(y + dy + ny, ny),
            "sp_2": cc, "tp": lax.rem(x + dx + 4, 4),
        }

    def remote(src, dst, send, recv, where):
        return pltpu.make_async_remote_copy(
            src_ref=src, dst_ref=dst, send_sem=send, recv_sem=recv, device_id=where, device_id_type=MESH
        )

    right, left = lax.rem(x + 1, 4), lax.rem(x + 3, 4)
    far = lax.rem(x + 2, 4)

    nsp = lax.rem(sp_index + 1, sp_count)
    psp = lax.rem(sp_index + sp_count - 1, sp_count)

    def of_sp(s):
        return {"sp_0": s // (2 * ny), "sp_1": lax.rem(s // 2, ny), "sp_2": lax.rem(s, 2), "tp": x}

    own_tok = pltpu.make_async_copy(tokens, tok.at[x], lsem.at[0])
    own_tok.start()
    ring = z * (1 - c) + y * c
    cross = y * (1 - c) + z * c
    core_row = pl.multiple_of(c * 16, 16)
    core_col = pl.multiple_of(c * pw, pw)
    stage_loads = []
    for m, src in enumerate((proj_x, gate_proj, proj_out)):
        slot = m if m < 2 else 2 + x
        loads = []
        for p in range(2):
            loads.append(pltpu.make_async_copy(src.at[:, pl.ds(p * pw, pw)], stage.at[slot, p], lsem.at[1 + 3 * m + p]))
        if m < 2:
            loads.append(pltpu.make_async_copy(
                src.at[:, pl.ds(core_col, pw)], wb.at[m, c, ring, cross, pl.ds(core_row, 16)], lsem.at[3 + 3 * m]))
        for load in loads:
            load.start()
        stage_loads.append(loads)
    gate_loads = [
        pltpu.make_async_copy(gate_recur, gr, gsem.at[0]),
        pltpu.make_async_copy(gate_input, gi, gsem.at[1]),
        pltpu.make_async_copy(taps_in, taps, gsem.at[2]),
    ]
    early_loads = [
        pltpu.make_async_copy(gain_in, gain, gsem.at[3]),
        pltpu.make_async_copy(param_in, decay_param, gsem.at[4]),
        pltpu.make_async_copy(shift_in, decay_shift, gsem.at[5]),
    ]
    for load in early_loads + gate_loads:
        load.start()

    barrier = pltpu.get_barrier_semaphore()
    peers = [at(dx=1), at(dx=2), at(dx=3)]
    peers += [at(dc=1)]
    peers += [at(dy=k, dc=d) for k in range(1, ny) for d in range(2)]
    peers += [at(dz=k, dc=d) for k in range(1, nz) for d in range(2)]
    peers += [of_sp(nsp), of_sp(psp)]
    for peer in peers:
        pl.semaphore_signal(barrier, inc=1, device_id=peer, device_id_type=MESH)
    pl.semaphore_wait(barrier, len(peers))

    def quarter(k):
        return remote(stage.at[2 + x], stage.at[2 + x], qsend.at[k - 1], qrecv.at[x], at(dx=k))

    def quarters_start():
        for load in stage_loads[2]:
            load.wait()
        for k in range(1, 4):
            quarter(k).start()

    def quarters_done():
        for k in range(1, 4):
            piece_in = stage.at[2 + lax.rem(x + k, 4)]
            pltpu.make_async_copy(piece_in, piece_in, qrecv.at[lax.rem(x + k, 4)]).wait()
        for m in range(2, 6):
            def put(m=m):
                wb[m, c, ring, cross, pl.ds(core_row, 16), :] = stage[m, c]
            given(m, cross, put)

    nq = wb.shape[3]
    hq = nq // 2
    last = nr // 2 - 1
    other = 1 - c
    away_r = z * c + y * (1 - c)
    away_q = y * c + z * (1 - c)

    def mine(m):
        return lax.rem(x + m, 2)

    def pieces(m):
        sends = [
            (y, [(stage.at[m, 0], wb.at[m, 0, z, y, pl.ds(core_row, 16)], at(dy=k, core=0)) for k in range(1, ny)]),
            (z, [(stage.at[m, 1], wb.at[m, 1, y, z, pl.ds(core_row, 16)], at(dz=k, core=1)) for k in range(1, nz)]),
            (away_q, [(stage.at[m, other], wb.at[m, other, away_r, away_q, pl.ds(core_row, 16)], at(dc=1))]),
        ]
        return sends

    def given(m, q, act):
        if m in HALVED:
            pl.when(q // hq == mine(m))(act)
        else:
            act()

    def first_phase(m):
        if m < 2:
            for load in stage_loads[m]:
                load.wait()
        for k, (q, sends) in enumerate(pieces(m)):
            def act(k=k, sends=sends):
                for src, dst, where in sends:
                    remote(src, dst, p1send.at[m, k], p1recv.at[m], where).start()
            given(m, q, act)

    def wait_rows(sem, count):
        ref = dummy.at[pl.ds(0, 16 * count)]
        pltpu.make_async_copy(ref, ref, sem).wait()

    def first_phase_done(m):
        if m in HALVED:
            own = cross // hq == mine(m)
            pl.when(own)(lambda: wait_rows(p1recv.at[m], nq - 1))
            pl.when(jnp.logical_not(own))(lambda: wait_rows(p1recv.at[m], nq))
        else:
            wait_rows(p1recv.at[m], 2 * nq - 1)

    def first_phase_sent(m):
        for k, (q, sends) in enumerate(pieces(m)):
            given(m, q, lambda k=k, sends=sends: wait_rows(p1send.at[m, k], len(sends)))

    def ring_at(step):
        return {
            "sp_0": lax.rem(z + (1 - c) * step + nr, nr) * (1 - c) + z * c,
            "sp_1": lax.rem(y + c * step + nr, nr) * c + y * (1 - c),
            "sp_2": c, "tp": x,
        }

    def half_block(m, block, part):
        return wb.at[m, c, block, pl.ds(part * hq, hq)]

    def ring_block(way, step):
        return lax.rem(ring - (1 if way == 0 else -1) * step + nr, nr)

    def ring_copy(m, way, step, part):
        ref = half_block(m, ring_block(way, step), mine(m) if m in HALVED else part)
        return remote(ref, ref, rsend.at[m, way, step, part], rrecv.at[m, way, step, part],
                      ring_at(1 if way == 0 else -1))

    def parts(m, way, step):
        if m in HALVED:
            return (0,)
        return (way, 1 - way) if step < last else (way,)

    def turn(m, way, step, act):
        if m in HALVED and step == last:
            pl.when(mine(m) == way)(act)
        else:
            act()

    def share(m, block, part):
        ref = half_block(m, block, mine(m) if m in HALVED else part)
        remote(ref, ref, dsend.at[m], drecv.at[m], at(dc=1)).start()
        if m in HALVED:
            remote(ref, ref, swapsend.at[m], swaprecv.at[m], at(dx=1 - 2 * (block // (nr // 2)))).start()

    def ring_first(m):
        first_phase_done(m)
        for k in range(len(parts(m, 0, 0))):
            for way in range(2):
                ring_copy(m, way, 0, parts(m, way, 0)[k]).start()
        for part in sorted(parts(m, 0, 0)):
            share(m, ring, part)

    def ring_step(m, step):
        for k in range(len(parts(m, 0, step))):
            for way in range(2):
                part = parts(m, way, step)[k]

                def act(way=way, part=part):
                    ring_copy(m, way, step, part).wait_recv()
                    if step < last and part in parts(m, way, step + 1):
                        turn(m, way, step + 1, lambda: ring_copy(m, way, step + 1, part).start())
                    share(m, ring_block(way, step + 1), part)

                turn(m, way, step, act)

    def ring_sent(m):
        for way in range(2):
            for step in range(last + 1):
                for part in parts(m, way, step):
                    turn(m, way, step, lambda: ring_copy(m, way, step, part).wait_send())
        if m in HALVED:
            ref = wb.at[m, c, :, pl.ds(0, hq)]
            pltpu.make_async_copy(ref, ref, swapsend.at[m]).wait()
        whole = wb.at[m, c]
        pltpu.make_async_copy(whole, whole, dsend.at[m]).wait()

    def swapped(m):
        if m in HALVED:
            ref = wb.at[m, c, :, pl.ds((1 - mine(m)) * hq, hq)]
            pltpu.make_async_copy(ref, ref, swaprecv.at[m]).wait()
            remote(ref, ref, dsend.at[m], drecv.at[m], at(dc=1)).start()

    def shared_done(m):
        whole = wb.at[m, 1 - c]
        pltpu.make_async_copy(whole, whole, drecv.at[m]).wait()

    def norm_part(b, base, count):
        g = gain_row

        @pl.loop(0, count // 32)
        def _(i):
            r = pl.ds(pl.multiple_of(base + i * 32, 32), 32)
            v = tok[b, r, :].astype(F32)
            s = lax.rsqrt(jnp.mean(v * v, axis=-1, keepdims=True) + 1e-06)
            nrm[b, r, :] = (v * s * g).astype(BF16)

    def weight(m, p):
        if p == 0:
            return wb[m, 0].reshape(-1, pw)
        return jnp.concatenate([wb[m, 1, :, k].reshape(-1, pw) for k in range(nq)], axis=0)

    def carry_on(place):
        for op in PLAN.get(place, ()):
            m = int(op[1:2] or 0)
            if op[0] == "P":
                first_phase(m)
            elif op[0] == "Q":
                quarters_done()
            elif op[0] == "S":
                swapped(m)
            elif op[2] == "0":
                ring_first(m)
            else:
                ring_step(m, int(op[2]) - 1)

    quarters_start()
    own_tok.wait()
    lo, hi = pl.ds(0, half), pl.ds(half, half)
    tok_a_r = remote(tok.at[x, lo], tok.at[x, lo], tsend.at[0], trecv.at[0], at(dx=1))
    tok_b_r = remote(tok.at[x, hi], tok.at[x, hi], tsend.at[1], trecv.at[1], at(dx=1))
    tok_b_l = remote(tok.at[x, hi], tok.at[x, hi], tsend.at[2], trecv.at[2], at(dx=-1))
    tok_a_l = remote(tok.at[x, lo], tok.at[x, lo], tsend.at[3], trecv.at[3], at(dx=-1))
    rel_a = remote(tok.at[left, lo], tok.at[left, lo], tsend.at[4], trecv.at[4], at(dx=1))
    rel_b = remote(tok.at[right, hi], tok.at[right, hi], tsend.at[5], trecv.at[5], at(dx=-1))
    for copy in (tok_a_r, tok_b_l, tok_b_r, tok_a_l):
        copy.start()

    first_phase(0)
    carry_on("start")
    for load in early_loads:
        load.wait()
    gain_rows = gain[...].astype(F32)
    gain_row = jnp.concatenate([gain_rows[k:k + 1] for k in range(gain_rows.shape[0])], axis=1)
    norm_part(x, 0, t)

    for h in range(heads):
        for k in range(rows // LANES):
            line = decay_shift[h:h + 1, k * LANES:(k + 1) * LANES]
            shiftc[h, k * LANES:(k + 1) * LANES, :] = jnp.transpose(jnp.broadcast_to(line, (LANES, LANES)))
    v = jnp.exp(-decay_param[...])
    rate = v * (1.0 - v * (1 / 2 - v * (1 / 3 - v * (1 / 4 - v * (1 / 5)))))
    rate8 = -8.0 * rate

    ring_first(0)
    carry_on("r0")
    ring_step(0, 0)
    tok_a_r.wait_recv()
    rel_a.start()
    tok_b_l.wait_recv()
    rel_b.start()
    carry_on("s0")
    ring_step(0, 1)
    carry_on("s1")
    norm_part(left, 0, half)
    norm_part(right, half, half)
    ring_step(0, 2)
    carry_on("s2")
    tok_b_r.wait_recv()
    tok_a_l.wait_recv()
    norm_part(left, half, half)
    norm_part(right, 0, half)
    rel_a.wait_recv()
    rel_b.wait_recv()
    norm_part(far, 0, t)
    ring_step(0, last)
    carry_on("last")
    shared_done(0)

    def branch_block(b):
        at_row = pl.ds(pl.multiple_of(8 + b * t, 8), t)
        for p in range(2):
            prod = jnp.dot(nrm[b], weight(0, p), preferred_element_type=F32)
            branch[at_row, p * pw:(p + 1) * pw] = prod.astype(BF16).astype(F32)

    @pl.loop(0, 4)
    def _(b):
        branch_block(b)

    carry_on("branch")

    tail_copy = remote(branch.at[pl.ds(rows, 8)], tail, xsem.at[0], xsem.at[1], of_sp(nsp))
    tail_copy.start()
    carry_on("far")
    for load in gate_loads:
        load.wait()

    tapf = taps[...].astype(F32)

    def gates(i):
        base = pl.multiple_of(i * t, t)
        win = branch[pl.ds(base, t + 8), :]
        acc = jnp.zeros((t, width), F32)
        for k in range(CONV):
            acc = acc + win[5 + k:5 + k + t] * tapf[k:k + 1]
        conv = acc.astype(BF16)
        at_row = pl.ds(base, t)
        for h in range(heads):
            cols = slice(h * HEAD, (h + 1) * HEAD)
            cb = conv[:, cols]
            cf = cb.astype(F32)
            ur = jnp.dot(cb, gr[h], preferred_element_type=F32)
            ui = jnp.dot(cb, gi[h], preferred_element_type=F32)
            recur = 1.0 / (1.0 + jnp.exp(-ur))
            inlet = 1.0 / (1.0 + jnp.exp(-ui))
            sh = shiftc[h, at_row, :]
            log_decay = recur * rate8[:, cols] + jnp.concatenate([sh] * (HEAD // LANES), axis=1)
            decay = jnp.exp(log_decay)
            u = 2.0 * log_decay
            near = u * (1.0 + u * (1 / 2) * (1.0 + u * (1 / 3) * (1.0 + u * (1 / 4) * (1.0 + u * (1 / 5) * (1.0 + u * (1 / 6))))))
            em1 = jnp.where(u > -0.25, near, decay * decay - 1.0)
            drive = jnp.sqrt(-em1) * inlet * cf
            for g in range(HEAD // LANES):
                lanes = slice(g * LANES, (g + 1) * LANES)
                for k in range(t // chunk):
                    part = slice(k * chunk, (k + 1) * chunk)
                    to = pl.ds(pl.multiple_of((i * (t // chunk) + k) * pitch, 8), chunk)
                    dec[h * (HEAD // LANES) + g, to, :] = decay[part, lanes]
                    drv[h * (HEAD // LANES) + g, to, :] = drive[part, lanes]

    gates(3)
    carry_on("g3")
    gates(2)
    carry_on("g2")
    gates(1)
    carry_on("g1")

    tail_copy.wait_recv()
    keep = jnp.where(sp_index > 0, 1.0, 0.0).astype(F32)
    branch[0:8, :] = tail[...] * keep
    gates(0)

    def scan_step(j, carried):
        pos = pl.ds(j, 8, stride=pitch)
        new = []
        for g in range(groups):
            prod, state = carried[g]
            a = dec[g, pos, :]
            b = drv[g, pos, :]
            state = a * state + b
            prod = prod * a
            dec[g, pos, :] = prod
            drv[g, pos, :] = state
            new.append((prod, state))
        return tuple(new)

    one, zero = jnp.ones((8, LANES), F32), jnp.zeros((8, LANES), F32)
    ends = lax.fori_loop(0, chunk, scan_step, ((one, zero),) * groups, unroll=4)
    for g in range(groups):
        prod, state = ends[g]
        pr, st = prod[0:1], state[0:1]
        for i in range(1, 8):
            st = prod[i:i + 1] * st + state[i:i + 1]
            pr = pr * prod[i:i + 1]
        mine1[0:1, g * LANES:(g + 1) * LANES] = pr
        mine1[1:2, g * LANES:(g + 1) * LANES] = st

    me1 = y * 2 + c
    n1 = 2 * ny
    firsts = [at(dc=1)] + [at(dy=k, dc=d) for k in range(1, ny) for d in range(2)]
    for peer in firsts:
        remote(mine1, s1.at[me1], xsem.at[2], xsem.at[3], peer).start()
    s1[me1] = mine1[...]

    def gating_block(b):
        for p in range(2):
            cols = slice(p * pw, (p + 1) * pw)
            prod = jnp.dot(nrm[b], weight(1, p), preferred_element_type=F32)
            v = prod.astype(BF16).astype(F32)
            inner = 0.7978845608028654 * (v + 0.044715 * (v * v * v))
            gel[pl.ds(pl.multiple_of(b * t, t), t), cols] = 0.5 * v * (1.0 + jnp.tanh(inner))

    def gating(first, end):
        if end > first:
            @pl.loop(first, end)
            def _(b):
                gating_block(b)

    carry_on("scan")
    if GATING:
        shared_done(1)
        gating(0, GATING)
    carry_on("w1")
    pltpu.make_async_copy(s1.at[pl.ds(0, n1 - 1)], s1.at[pl.ds(0, n1 - 1)], xsem.at[3]).wait()
    p_all, s_all = s1[0, 0:1], s1[0, 1:2]
    p_in = jnp.where(me1 > 0, p_all, 1.0)
    s_in = jnp.where(me1 > 0, s_all, 0.0)
    for k in range(1, n1):
        s_all = s1[k, 0:1] * s_all + s1[k, 1:2]
        p_all = p_all * s1[k, 0:1]
        p_in = jnp.where(k < me1, p_all, p_in)
        s_in = jnp.where(k < me1, s_all, s_in)
    mine2[0:1, :] = p_all
    mine2[1:2, :] = s_all
    for k in range(1, nz):
        remote(mine2, s2.at[z], xsem.at[4], xsem.at[5], at(dz=k)).start()
    s2[z] = mine2[...]

    carry_on("f1")
    if not GATING:
        shared_done(1)
    gating(GATING, 4)
    carry_on("w2")
    pltpu.make_async_copy(s2.at[pl.ds(0, nz - 1)], s2.at[pl.ds(0, nz - 1)], xsem.at[5]).wait()
    s_plane = jnp.zeros((1, width), F32)
    for k in range(nz - 1):
        s_plane = jnp.where(k < z, s2[k, 0:1] * s_plane + s2[k, 1:2], s_plane)
    carry = p_in * s_plane + s_in
    for g in range(groups):
        lanes = slice(g * LANES, (g + 1) * LANES)
        prod, state = ends[g]
        now = carry[:, lanes]
        for i in range(8):
            cin[g, i:i + 1, :] = now
            now = prod[i:i + 1] * now + state[i:i + 1]

    def mixed_block(b):
        for g in range(groups):
            parts = []
            lanes = slice(g * LANES, (g + 1) * LANES)
            for i in range(t // chunk):
                at_chunk = b * (t // chunk) + i
                r = pl.ds(pl.multiple_of(at_chunk * pitch, 8), chunk)
                st = drv[g, r, :] + dec[g, r, :] * cin[g, pl.ds(at_chunk, 1), :]
                parts.append(st * gel[pl.ds(pl.multiple_of(at_chunk * chunk, chunk), chunk), lanes])
            mx[b, lanes, :] = jnp.transpose(jnp.concatenate(parts, axis=0)).astype(BF16)

    half_w = width // 2
    wlo, whi = pl.ds(0, half_w), pl.ds(half_w, half_w)
    mixed_block(far)
    far_a = remote(mx.at[far, wlo], relay.at[0], osend.at[0], orecv.at[0], at(dx=1))
    far_b = remote(mx.at[far, whi], relay.at[1], osend.at[1], orecv.at[1], at(dx=-1))
    far_a.start()
    far_b.start()
    mixed_block(right)
    to_right = remote(mx.at[right], mixed.at[x], osend.at[2], orecv.at[2], at(dx=1))
    to_right.start()
    mixed_block(left)
    to_left = remote(mx.at[left], mixed.at[x], osend.at[3], orecv.at[3], at(dx=-1))
    to_left.start()
    mixed_block(x)
    carry_on("mix")
    far_a.wait_recv()
    pass_a = remote(relay.at[0], mixed.at[left, wlo], osend.at[4], orecv.at[4], at(dx=1))
    pass_a.start()
    far_b.wait_recv()
    pass_b = remote(relay.at[1], mixed.at[right, whi], osend.at[5], orecv.at[5], at(dx=-1))
    pass_b.start()
    carry_on("rel")

    tile = ny * 32

    def out_tile(q, source, n):
        w0 = wb[2 + q, 0, n].reshape(tile, pw)
        w1 = wb[2 + q, 1, :, n].reshape(tile, pw)
        r = jnp.dot(w0, source[:pw, :], preferred_element_type=F32)
        return r + jnp.dot(w1, source[pw:, :], preferred_element_type=F32)

    for m in range(2, 6):
        shared_done(m)
    @pl.loop(0, nz, unroll=4)
    def _(n):
        acc[n] = out_tile(x, mx[x], n)

    to_right.wait_recv()
    to_left.wait_recv()

    @pl.loop(0, nz, unroll=4)
    def _(n):
        acc[n] = acc[n] + out_tile(left, mixed[left], n) + out_tile(right, mixed[right], n)

    pass_a.wait_recv()
    pass_b.wait_recv()
    leave = []
    for k in range(2):
        @pl.loop(k * (nz // 2), (k + 1) * (nz // 2), unroll=nz // 2)
        def _(n):
            total = acc[n] + out_tile(far, mixed[far], n)
            outv[:, pl.ds(pl.multiple_of(n * tile, tile), tile)] = jnp.transpose(total).astype(BF16)

        side = pl.ds(k * (nz // 2) * tile, (nz // 2) * tile)
        leave.append(pltpu.make_async_copy(outv.at[:, side], out.at[:, side], lsem.at[k]))
        leave[k].start()

    for copy in (tok_a_r, tok_b_r, tok_b_l, tok_a_l, rel_a, rel_b, tail_copy, far_a, far_b, to_right, to_left, pass_a, pass_b,
                 quarter(1), quarter(2), quarter(3)):
        copy.wait_send()
    for m in range(6):
        first_phase_sent(m)
        ring_sent(m)
    pltpu.make_async_copy(s1.at[pl.ds(0, n1 - 1)], s1.at[pl.ds(0, n1 - 1)], xsem.at[2]).wait()
    pltpu.make_async_copy(s2.at[pl.ds(0, nz - 1)], s2.at[pl.ds(0, nz - 1)], xsem.at[4]).wait()
    for copy in leave:
        copy.wait()


def on_device(
    nz, ny,
    tokens, norm_gain, proj_x, gate_projection, conv_taps, gate_recur, gate_input, decay_param, decay_shift, proj_out,
):
    t, d = tokens.shape
    width = proj_x.shape[1]
    pw = width // 2
    groups = width // LANES
    heads = width // HEAD
    rows = 4 * t
    last = nz // 2
    dma = pltpu.SemaphoreType.DMA
    any_ = pl.BlockSpec(memory_space=pl.ANY)
    scratch = [
        pltpu.VMEM((4, t, d), BF16),
        pltpu.VMEM((4, t, d), BF16),
        pltpu.VMEM((6, 2, 16, pw), BF16),
        pltpu.VMEM((6, 2, nz, ny, 32, pw), BF16),
        pltpu.VMEM(gate_recur.shape, BF16),
        pltpu.VMEM(gate_input.shape, BF16),
        pltpu.VMEM((rows + 8, width), F32),
        pltpu.VMEM((groups, rows + 136, LANES), F32),
        pltpu.VMEM((groups, rows + 136, LANES), F32),
        pltpu.VMEM((heads, rows, LANES), F32),
        pltpu.VMEM((rows, width), F32),
        pltpu.VMEM((4, width, t), BF16),
        pltpu.VMEM((8, width), F32),
        pltpu.VMEM((2, width), F32),
        pltpu.VMEM((2 * ny, 2, width), F32),
        pltpu.VMEM((2, width), F32),
        pltpu.VMEM((nz, 2, width), F32),
        pltpu.VMEM((groups, 8, LANES), F32),
        pltpu.VMEM(((ny + nz - 1) * 16, pw), BF16),
        pltpu.VMEM((t, d), BF16),
        pltpu.VMEM((4, width, t), BF16),
        pltpu.VMEM((2, width // 2, t), BF16),
        pltpu.VMEM((nz, ny * 32, t), F32),
        pltpu.VMEM((d // LANES, LANES), BF16),
        pltpu.VMEM(conv_taps.shape, BF16),
        pltpu.VMEM((1, width), F32),
        pltpu.VMEM(decay_shift.shape, F32),
        dma((10,)), dma((6,)), dma((6,)), dma((6,)), dma((6, 3)), dma((6,)),
        dma((6, 2, last, 2)), dma((6, 2, last, 2)), dma((6,)), dma((6,)), dma((6,)), dma((6,)), dma((6,)), dma((3,)), dma((4,)),
        dma((6,)), dma((6,)),
    ]
    return pl.pallas_call(
        functools.partial(body, nz, ny),
        out_shape=jax.ShapeDtypeStruct((t, d), BF16),
        in_specs=[any_] * 10,
        out_specs=any_,
        scratch_shapes=scratch,
        compiler_params=pltpu.CompilerParams(
            collective_id=0, has_side_effects=True, vmem_limit_bytes=60 * 1024 * 1024
        ),
        name="recurrence",
    )(
        tokens, norm_gain.reshape(-1, LANES), proj_x, gate_projection, conv_taps, gate_recur, gate_input,
        decay_param.reshape(1, -1), decay_shift, jnp.transpose(proj_out),
    )


def build(mesh, nz, ny):
    split = Mesh(mesh.devices.reshape(nz, ny, 2, mesh.shape["tp"]), ("sp_0", "sp_1", "sp_2", "tp"))
    in_specs = (
        P(SP_TP, None),
        P(),
        P(SP, "tp"),
        P(SP, "tp"),
        P(None, "tp"),
        P("tp", None, None),
        P("tp", None, None),
        P("tp"),
        P("tp", SP),
        P("tp", SP),
    )
    out_specs = P(SP_TP, None)
    return jax.shard_map(
        functools.partial(on_device, nz, ny), mesh=split, in_specs=in_specs, out_specs=out_specs, check_vma=False
    )


def solution(mesh):
    return build(mesh, 8, 8)
```

```python
import functools

import jax
import jax.numpy as jnp
from jax import lax
from jax.experimental import pallas as pl
from jax.experimental.pallas import tpu as pltpu
from jax.sharding import Mesh
from jax.sharding import PartitionSpec as P

HEAD = 256
CONV = 4
SP = ("sp_0", "sp_1", "sp_2")
SP_TP = ("sp_0", "sp_1", "sp_2", "tp")
MESH = pl.DeviceIdType.MESH
F32 = jnp.float32
BF16 = jnp.bfloat16
HALVED = (4, 5)
PLAN = {
    "start": ("P1",),
    "r0": ("R10", "Q", "P4", "P5",),
    "s0": ("R11",),
    "s1": ("R12", "P2",),
    "s2": ("R13", "R40", "R50", "P3",),
    "last": ("R14", "R41", "R51", "R20",),
    "far": ("R42", "R52", "R30",),
    "g2": ("R21",),
    "scan": ("R43", "R53", "R31",),
    "w1": ("R22",),
    "f1": ("R32", "R44", "R54",),
    "w2": ("R23", "R33",),
    "mix": ("R24", "R34", "S4", "S5",),
}
GATING = 2
LANES = 128


def body(
    nz, ny,
    tokens, gain_in, proj_x, gate_proj, taps_in, gate_recur, gate_input, param_in, shift_in, proj_out,
    out,
    tok, nrm, stage, wb, gr, gi, branch, dec, drv, shiftc, gel, mx, tail,
    mine1, s1, mine2, s2, cin, dummy, outv,
    mixed, relay, acc,
    gain, taps, decay_param, decay_shift,
    lsem, gsem, tsend, trecv, p1send, p1recv, rsend, rrecv, dsend, drecv, xsem, osend, orecv, qsend, qrecv, swapsend, swaprecv,
):
    z, y, c, x = (lax.axis_index(a) for a in SP_TP)
    t = tok.shape[1]
    half = t // 2
    rows = 4 * t
    chunk = rows // 8
    pitch = chunk + 8
    width = 2 * wb.shape[-1]
    groups = width // LANES
    heads = width // HEAD
    pw = width // 2
    nr = wb.shape[2]
    sp_index = (z * ny + y) * 2 + c
    sp_count = nz * ny * 2

    def at(dz=0, dy=0, dc=None, dx=0, core=None):
        cc = c if dc is None else lax.rem(c + dc, 2)
        cc = cc if core is None else core
        return {
            "sp_0": lax.rem(z + dz + nz, nz), "sp_1": lax.rem(y + dy + ny, ny),
            "sp_2": cc, "tp": lax.rem(x + dx + 4, 4),
        }

    def remote(src, dst, send, recv, where):
        return pltpu.make_async_remote_copy(
            src_ref=src, dst_ref=dst, send_sem=send, recv_sem=recv, device_id=where, device_id_type=MESH
        )

    right, left = lax.rem(x + 1, 4), lax.rem(x + 3, 4)
    far = lax.rem(x + 2, 4)

    nsp = lax.rem(sp_index + 1, sp_count)
    psp = lax.rem(sp_index + sp_count - 1, sp_count)

    def of_sp(s):
        return {"sp_0": s // (2 * ny), "sp_1": lax.rem(s // 2, ny), "sp_2": lax.rem(s, 2), "tp": x}

    own_tok = pltpu.make_async_copy(tokens, tok.at[x], lsem.at[0])
    own_tok.start()
    ring = z * (1 - c) + y * c
    cross = y * (1 - c) + z * c
    core_row = pl.multiple_of(c * 16, 16)
    core_col = pl.multiple_of(c * pw, pw)
    stage_loads = []
    for m, src in enumerate((proj_x, gate_proj, proj_out)):
        slot = m if m < 2 else 2 + x
        loads = []
        for p in range(2):
            loads.append(pltpu.make_async_copy(src.at[:, pl.ds(p * pw, pw)], stage.at[slot, p], lsem.at[1 + 3 * m + p]))
        if m < 2:
            loads.append(pltpu.make_async_copy(
                src.at[:, pl.ds(core_col, pw)], wb.at[m, c, ring, cross, pl.ds(core_row, 16)], lsem.at[3 + 3 * m]))
        for load in loads:
            load.start()
        stage_loads.append(loads)
    gate_loads = [
        pltpu.make_async_copy(gate_recur, gr, gsem.at[0]),
        pltpu.make_async_copy(gate_input, gi, gsem.at[1]),
        pltpu.make_async_copy(taps_in, taps, gsem.at[2]),
    ]
    early_loads = [
        pltpu.make_async_copy(gain_in, gain, gsem.at[3]),
        pltpu.make_async_copy(param_in, decay_param, gsem.at[4]),
        pltpu.make_async_copy(shift_in, decay_shift, gsem.at[5]),
    ]
    for load in early_loads + gate_loads:
        load.start()

    barrier = pltpu.get_barrier_semaphore()
    peers = [at(dx=1), at(dx=2), at(dx=3)]
    peers += [at(dc=1)]
    peers += [at(dy=k, dc=d) for k in range(1, ny) for d in range(2)]
    peers += [at(dz=k, dc=d) for k in range(1, nz) for d in range(2)]
    peers += [of_sp(nsp), of_sp(psp)]
    for peer in peers:
        pl.semaphore_signal(barrier, inc=1, device_id=peer, device_id_type=MESH)
    pl.semaphore_wait(barrier, len(peers))

    def quarter(k):
        return remote(stage.at[2 + x], stage.at[2 + x], qsend.at[k - 1], qrecv.at[x], at(dx=k))

    def quarters_start():
        for load in stage_loads[2]:
            load.wait()
        for k in range(1, 4):
            quarter(k).start()

    def quarters_done():
        for k in range(1, 4):
            piece_in = stage.at[2 + lax.rem(x + k, 4)]
            pltpu.make_async_copy(piece_in, piece_in, qrecv.at[lax.rem(x + k, 4)]).wait()
        for m in range(2, 6):
            def put(m=m):
                wb[m, c, ring, cross, pl.ds(core_row, 16), :] = stage[m, c]
            given(m, cross, put)

    nq = wb.shape[3]
    hq = nq // 2
    last = nr // 2 - 1
    other = 1 - c
    away_r = z * c + y * (1 - c)
    away_q = y * c + z * (1 - c)

    def mine(m):
        return lax.rem(x + m, 2)

    def pieces(m):
        sends = [
            (y, [(stage.at[m, 0], wb.at[m, 0, z, y, pl.ds(core_row, 16)], at(dy=k, core=0)) for k in range(1, ny)]),
            (z, [(stage.at[m, 1], wb.at[m, 1, y, z, pl.ds(core_row, 16)], at(dz=k, core=1)) for k in range(1, nz)]),
            (away_q, [(stage.at[m, other], wb.at[m, other, away_r, away_q, pl.ds(core_row, 16)], at(dc=1))]),
        ]
        return sends

    def given(m, q, act):
        if m in HALVED:
            pl.when(q // hq == mine(m))(act)
        else:
            act()

    def first_phase(m):
        if m < 2:
            for load in stage_loads[m]:
                load.wait()
        for k, (q, sends) in enumerate(pieces(m)):
            def act(k=k, sends=sends):
                for src, dst, where in sends:
                    remote(src, dst, p1send.at[m, k], p1recv.at[m], where).start()
            given(m, q, act)

    def wait_rows(sem, count):
        ref = dummy.at[pl.ds(0, 16 * count)]
        pltpu.make_async_copy(ref, ref, sem).wait()

    def first_phase_done(m):
        if m in HALVED:
            own = cross // hq == mine(m)
            pl.when(own)(lambda: wait_rows(p1recv.at[m], nq - 1))
            pl.when(jnp.logical_not(own))(lambda: wait_rows(p1recv.at[m], nq))
        else:
            wait_rows(p1recv.at[m], 2 * nq - 1)

    def first_phase_sent(m):
        for k, (q, sends) in enumerate(pieces(m)):
            given(m, q, lambda k=k, sends=sends: wait_rows(p1send.at[m, k], len(sends)))

    def ring_at(step):
        return {
            "sp_0": lax.rem(z + (1 - c) * step + nr, nr) * (1 - c) + z * c,
            "sp_1": lax.rem(y + c * step + nr, nr) * c + y * (1 - c),
            "sp_2": c, "tp": x,
        }

    def half_block(m, block, part):
        return wb.at[m, c, block, pl.ds(part * hq, hq)]

    def ring_block(way, step):
        return lax.rem(ring - (1 if way == 0 else -1) * step + nr, nr)

    def ring_copy(m, way, step, part):
        ref = half_block(m, ring_block(way, step), mine(m) if m in HALVED else part)
        return remote(ref, ref, rsend.at[m, way, step, part], rrecv.at[m, way, step, part],
                      ring_at(1 if way == 0 else -1))

    def parts(m, way, step):
        if m in HALVED:
            return (0,)
        return (way, 1 - way) if step < last else (way,)

    def turn(m, way, step, act):
        if m in HALVED and step == last:
            pl.when(mine(m) == way)(act)
        else:
            act()

    def share(m, block, part):
        ref = half_block(m, block, mine(m) if m in HALVED else part)
        remote(ref, ref, dsend.at[m], drecv.at[m], at(dc=1)).start()
        if m in HALVED:
            remote(ref, ref, swapsend.at[m], swaprecv.at[m], at(dx=1 - 2 * (block // (nr // 2)))).start()

    def ring_first(m):
        first_phase_done(m)
        for k in range(len(parts(m, 0, 0))):
            for way in range(2):
                ring_copy(m, way, 0, parts(m, way, 0)[k]).start()
        for part in sorted(parts(m, 0, 0)):
            share(m, ring, part)

    def ring_step(m, step):
        for k in range(len(parts(m, 0, step))):
            for way in range(2):
                part = parts(m, way, step)[k]

                def act(way=way, part=part):
                    ring_copy(m, way, step, part).wait_recv()
                    if step < last and part in parts(m, way, step + 1):
                        turn(m, way, step + 1, lambda: ring_copy(m, way, step + 1, part).start())
                    share(m, ring_block(way, step + 1), part)

                turn(m, way, step, act)

    def ring_sent(m):
        for way in range(2):
            for step in range(last + 1):
                for part in parts(m, way, step):
                    turn(m, way, step, lambda: ring_copy(m, way, step, part).wait_send())
        if m in HALVED:
            ref = wb.at[m, c, :, pl.ds(0, hq)]
            pltpu.make_async_copy(ref, ref, swapsend.at[m]).wait()
        whole = wb.at[m, c]
        pltpu.make_async_copy(whole, whole, dsend.at[m]).wait()

    def swapped(m):
        if m in HALVED:
            ref = wb.at[m, c, :, pl.ds((1 - mine(m)) * hq, hq)]
            pltpu.make_async_copy(ref, ref, swaprecv.at[m]).wait()
            remote(ref, ref, dsend.at[m], drecv.at[m], at(dc=1)).start()

    def shared_done(m):
        whole = wb.at[m, 1 - c]
        pltpu.make_async_copy(whole, whole, drecv.at[m]).wait()

    def norm_part(b, base, count):
        g = gain_row

        @pl.loop(0, count // 32)
        def _(i):
            r = pl.ds(pl.multiple_of(base + i * 32, 32), 32)
            v = tok[b, r, :].astype(F32)
            s = lax.rsqrt(jnp.mean(v * v, axis=-1, keepdims=True) + 1e-06)
            nrm[b, r, :] = (v * s * g).astype(BF16)

    def weight(m, p):
        if p == 0:
            return wb[m, 0].reshape(-1, pw)
        return jnp.concatenate([wb[m, 1, :, k].reshape(-1, pw) for k in range(nq)], axis=0)

    def carry_on(place):
        for op in PLAN.get(place, ()):
            m = int(op[1:2] or 0)
            if op[0] == "P":
                first_phase(m)
            elif op[0] == "Q":
                quarters_done()
            elif op[0] == "S":
                swapped(m)
            elif op[2] == "0":
                ring_first(m)
            else:
                ring_step(m, int(op[2]) - 1)

    quarters_start()
    own_tok.wait()
    lo, hi = pl.ds(0, half), pl.ds(half, half)
    tok_a_r = remote(tok.at[x, lo], tok.at[x, lo], tsend.at[0], trecv.at[0], at(dx=1))
    tok_b_r = remote(tok.at[x, hi], tok.at[x, hi], tsend.at[1], trecv.at[1], at(dx=1))
    tok_b_l = remote(tok.at[x, hi], tok.at[x, hi], tsend.at[2], trecv.at[2], at(dx=-1))
    tok_a_l = remote(tok.at[x, lo], tok.at[x, lo], tsend.at[3], trecv.at[3], at(dx=-1))
    rel_a = remote(tok.at[left, lo], tok.at[left, lo], tsend.at[4], trecv.at[4], at(dx=1))
    rel_b = remote(tok.at[right, hi], tok.at[right, hi], tsend.at[5], trecv.at[5], at(dx=-1))
    for copy in (tok_a_r, tok_b_l, tok_b_r, tok_a_l):
        copy.start()

    first_phase(0)
    carry_on("start")
    for load in early_loads:
        load.wait()
    gain_rows = gain[...].astype(F32)
    gain_row = jnp.concatenate([gain_rows[k:k + 1] for k in range(gain_rows.shape[0])], axis=1)
    norm_part(x, 0, t)

    for h in range(heads):
        for k in range(rows // LANES):
            line = decay_shift[h:h + 1, k * LANES:(k + 1) * LANES]
            shiftc[h, k * LANES:(k + 1) * LANES, :] = jnp.transpose(jnp.broadcast_to(line, (LANES, LANES)))
    v = jnp.exp(-decay_param[...])
    rate = v * (1.0 - v * (1 / 2 - v * (1 / 3 - v * (1 / 4 - v * (1 / 5)))))
    rate8 = -8.0 * rate

    ring_first(0)
    carry_on("r0")
    ring_step(0, 0)
    tok_a_r.wait_recv()
    rel_a.start()
    tok_b_l.wait_recv()
    rel_b.start()
    carry_on("s0")
    ring_step(0, 1)
    carry_on("s1")
    norm_part(left, 0, half)
    norm_part(right, half, half)
    ring_step(0, 2)
    carry_on("s2")
    tok_b_r.wait_recv()
    tok_a_l.wait_recv()
    norm_part(left, half, half)
    norm_part(right, 0, half)
    rel_a.wait_recv()
    rel_b.wait_recv()
    norm_part(far, 0, t)
    ring_step(0, last)
    carry_on("last")
    shared_done(0)

    def branch_block(b):
        at_row = pl.ds(pl.multiple_of(8 + b * t, 8), t)
        for p in range(2):
            prod = jnp.dot(nrm[b], weight(0, p), preferred_element_type=F32)
            branch[at_row, p * pw:(p + 1) * pw] = prod.astype(BF16).astype(F32)

    @pl.loop(0, 4)
    def _(b):
        branch_block(b)

    carry_on("branch")

    tail_copy = remote(branch.at[pl.ds(rows, 8)], tail, xsem.at[0], xsem.at[1], of_sp(nsp))
    tail_copy.start()
    carry_on("far")
    for load in gate_loads:
        load.wait()

    tapf = taps[...].astype(F32)

    def gates(i):
        base = pl.multiple_of(i * t, t)
        win = branch[pl.ds(base, t + 8), :]
        acc = jnp.zeros((t, width), F32)
        for k in range(CONV):
            acc = acc + win[5 + k:5 + k + t] * tapf[k:k + 1]
        conv = acc.astype(BF16)
        at_row = pl.ds(base, t)
        for h in range(heads):
            cols = slice(h * HEAD, (h + 1) * HEAD)
            cb = conv[:, cols]
            cf = cb.astype(F32)
            ur = jnp.dot(cb, gr[h], preferred_element_type=F32)
            ui = jnp.dot(cb, gi[h], preferred_element_type=F32)
            recur = 1.0 / (1.0 + jnp.exp(-ur))
            inlet = 1.0 / (1.0 + jnp.exp(-ui))
            sh = shiftc[h, at_row, :]
            log_decay = recur * rate8[:, cols] + jnp.concatenate([sh] * (HEAD // LANES), axis=1)
            decay = jnp.exp(log_decay)
            u = 2.0 * log_decay
            near = u * (1.0 + u * (1 / 2) * (1.0 + u * (1 / 3) * (1.0 + u * (1 / 4) * (1.0 + u * (1 / 5) * (1.0 + u * (1 / 6))))))
            em1 = jnp.where(u > -0.25, near, decay * decay - 1.0)
            drive = jnp.sqrt(-em1) * inlet * cf
            for g in range(HEAD // LANES):
                lanes = slice(g * LANES, (g + 1) * LANES)
                for k in range(t // chunk):
                    part = slice(k * chunk, (k + 1) * chunk)
                    to = pl.ds(pl.multiple_of((i * (t // chunk) + k) * pitch, 8), chunk)
                    dec[h * (HEAD // LANES) + g, to, :] = decay[part, lanes]
                    drv[h * (HEAD // LANES) + g, to, :] = drive[part, lanes]

    gates(3)
    carry_on("g3")
    gates(2)
    carry_on("g2")
    gates(1)
    carry_on("g1")

    tail_copy.wait_recv()
    keep = jnp.where(sp_index > 0, 1.0, 0.0).astype(F32)
    branch[0:8, :] = tail[...] * keep
    gates(0)

    def scan_step(j, carried):
        pos = pl.ds(j, 8, stride=pitch)
        new = []
        for g in range(groups):
            prod, state = carried[g]
            a = dec[g, pos, :]
            b = drv[g, pos, :]
            state = a * state + b
            prod = prod * a
            dec[g, pos, :] = prod
            drv[g, pos, :] = state
            new.append((prod, state))
        return tuple(new)

    one, zero = jnp.ones((8, LANES), F32), jnp.zeros((8, LANES), F32)
    ends = lax.fori_loop(0, chunk, scan_step, ((one, zero),) * groups, unroll=4)
    for g in range(groups):
        prod, state = ends[g]
        pr, st = prod[0:1], state[0:1]
        for i in range(1, 8):
            st = prod[i:i + 1] * st + state[i:i + 1]
            pr = pr * prod[i:i + 1]
        mine1[0:1, g * LANES:(g + 1) * LANES] = pr
        mine1[1:2, g * LANES:(g + 1) * LANES] = st

    me1 = y * 2 + c
    n1 = 2 * ny
    firsts = [at(dc=1)] + [at(dy=k, dc=d) for k in range(1, ny) for d in range(2)]
    for peer in firsts:
        remote(mine1, s1.at[me1], xsem.at[2], xsem.at[3], peer).start()
    s1[me1] = mine1[...]

    def gating_block(b):
        for p in range(2):
            cols = slice(p * pw, (p + 1) * pw)
            prod = jnp.dot(nrm[b], weight(1, p), preferred_element_type=F32)
            v = prod.astype(BF16).astype(F32)
            inner = 0.7978845608028654 * (v + 0.044715 * (v * v * v))
            gel[pl.ds(pl.multiple_of(b * t, t), t), cols] = 0.5 * v * (1.0 + jnp.tanh(inner))

    def gating(first, end):
        if end > first:
            @pl.loop(first, end)
            def _(b):
                gating_block(b)

    carry_on("scan")
    if GATING:
        shared_done(1)
        gating(0, GATING)
    carry_on("w1")
    pltpu.make_async_copy(s1.at[pl.ds(0, n1 - 1)], s1.at[pl.ds(0, n1 - 1)], xsem.at[3]).wait()
    p_all, s_all = s1[0, 0:1], s1[0, 1:2]
    p_in = jnp.where(me1 > 0, p_all, 1.0)
    s_in = jnp.where(me1 > 0, s_all, 0.0)
    for k in range(1, n1):
        s_all = s1[k, 0:1] * s_all + s1[k, 1:2]
        p_all = p_all * s1[k, 0:1]
        p_in = jnp.where(k < me1, p_all, p_in)
        s_in = jnp.where(k < me1, s_all, s_in)
    mine2[0:1, :] = p_all
    mine2[1:2, :] = s_all
    for k in range(1, nz):
        remote(mine2, s2.at[z], xsem.at[4], xsem.at[5], at(dz=k)).start()
    s2[z] = mine2[...]

    carry_on("f1")
    if not GATING:
        shared_done(1)
    gating(GATING, 4)
    carry_on("w2")
    pltpu.make_async_copy(s2.at[pl.ds(0, nz - 1)], s2.at[pl.ds(0, nz - 1)], xsem.at[5]).wait()
    s_plane = jnp.zeros((1, width), F32)
    for k in range(nz - 1):
        s_plane = jnp.where(k < z, s2[k, 0:1] * s_plane + s2[k, 1:2], s_plane)
    carry = p_in * s_plane + s_in
    for g in range(groups):
        lanes = slice(g * LANES, (g + 1) * LANES)
        prod, state = ends[g]
        now = carry[:, lanes]
        for i in range(8):
            cin[g, i:i + 1, :] = now
            now = prod[i:i + 1] * now + state[i:i + 1]

    def mixed_block(b):
        for g in range(groups):
            parts = []
            lanes = slice(g * LANES, (g + 1) * LANES)
            for i in range(t // chunk):
                at_chunk = b * (t // chunk) + i
                r = pl.ds(pl.multiple_of(at_chunk * pitch, 8), chunk)
                st = drv[g, r, :] + dec[g, r, :] * cin[g, pl.ds(at_chunk, 1), :]
                parts.append(st * gel[pl.ds(pl.multiple_of(at_chunk * chunk, chunk), chunk), lanes])
            mx[b, lanes, :] = jnp.transpose(jnp.concatenate(parts, axis=0)).astype(BF16)

    half_w = width // 2
    wlo, whi = pl.ds(0, half_w), pl.ds(half_w, half_w)
    mixed_block(far)
    far_a = remote(mx.at[far, wlo], relay.at[0], osend.at[0], orecv.at[0], at(dx=1))
    far_b = remote(mx.at[far, whi], relay.at[1], osend.at[1], orecv.at[1], at(dx=-1))
    far_a.start()
    far_b.start()
    mixed_block(right)
    to_right = remote(mx.at[right], mixed.at[x], osend.at[2], orecv.at[2], at(dx=1))
    to_right.start()
    mixed_block(left)
    to_left = remote(mx.at[left], mixed.at[x], osend.at[3], orecv.at[3], at(dx=-1))
    to_left.start()
    mixed_block(x)
    carry_on("mix")
    far_a.wait_recv()
    pass_a = remote(relay.at[0], mixed.at[left, wlo], osend.at[4], orecv.at[4], at(dx=1))
    pass_a.start()
    far_b.wait_recv()
    pass_b = remote(relay.at[1], mixed.at[right, whi], osend.at[5], orecv.at[5], at(dx=-1))
    pass_b.start()
    carry_on("rel")

    tile = ny * 32

    def out_tile(q, source, n):
        w0 = wb[2 + q, 0, n].reshape(tile, pw)
        w1 = wb[2 + q, 1, :, n].reshape(tile, pw)
        r = jnp.dot(w0, source[:pw, :], preferred_element_type=F32)
        return r + jnp.dot(w1, source[pw:, :], preferred_element_type=F32)

    for m in range(2, 6):
        shared_done(m)
    @pl.loop(0, nz, unroll=4)
    def _(n):
        acc[n] = out_tile(x, mx[x], n)

    to_right.wait_recv()
    to_left.wait_recv()

    @pl.loop(0, nz, unroll=4)
    def _(n):
        acc[n] = acc[n] + out_tile(left, mixed[left], n) + out_tile(right, mixed[right], n)

    pass_a.wait_recv()
    pass_b.wait_recv()
    leave = []
    for k in range(2):
        @pl.loop(k * (nz // 2), (k + 1) * (nz // 2), unroll=nz // 2)
        def _(n):
            total = acc[n] + out_tile(far, mixed[far], n)
            outv[:, pl.ds(pl.multiple_of(n * tile, tile), tile)] = jnp.transpose(total).astype(BF16)

        side = pl.ds(k * (nz // 2) * tile, (nz // 2) * tile)
        leave.append(pltpu.make_async_copy(outv.at[:, side], out.at[:, side], lsem.at[k]))
        leave[k].start()

    for copy in (tok_a_r, tok_b_r, tok_b_l, tok_a_l, rel_a, rel_b, tail_copy, far_a, far_b, to_right, to_left, pass_a, pass_b,
                 quarter(1), quarter(2), quarter(3)):
        copy.wait_send()
    for m in range(6):
        first_phase_sent(m)
        ring_sent(m)
    pltpu.make_async_copy(s1.at[pl.ds(0, n1 - 1)], s1.at[pl.ds(0, n1 - 1)], xsem.at[2]).wait()
    pltpu.make_async_copy(s2.at[pl.ds(0, nz - 1)], s2.at[pl.ds(0, nz - 1)], xsem.at[4]).wait()
    for copy in leave:
        copy.wait()


def on_device(
    nz, ny,
    tokens, norm_gain, proj_x, gate_projection, conv_taps, gate_recur, gate_input, decay_param, decay_shift, proj_out,
):
    t, d = tokens.shape
    width = proj_x.shape[1]
    pw = width // 2
    groups = width // LANES
    heads = width // HEAD
    rows = 4 * t
    last = nz // 2
    dma = pltpu.SemaphoreType.DMA
    any_ = pl.BlockSpec(memory_space=pl.ANY)
    scratch = [
        pltpu.VMEM((4, t, d), BF16),
        pltpu.VMEM((4, t, d), BF16),
        pltpu.VMEM((6, 2, 16, pw), BF16),
        pltpu.VMEM((6, 2, nz, ny, 32, pw), BF16),
        pltpu.VMEM(gate_recur.shape, BF16),
        pltpu.VMEM(gate_input.shape, BF16),
        pltpu.VMEM((rows + 8, width), F32),
        pltpu.VMEM((groups, rows + 136, LANES), F32),
        pltpu.VMEM((groups, rows + 136, LANES), F32),
        pltpu.VMEM((heads, rows, LANES), F32),
        pltpu.VMEM((rows, width), F32),
        pltpu.VMEM((4, width, t), BF16),
        pltpu.VMEM((8, width), F32),
        pltpu.VMEM((2, width), F32),
        pltpu.VMEM((2 * ny, 2, width), F32),
        pltpu.VMEM((2, width), F32),
        pltpu.VMEM((nz, 2, width), F32),
        pltpu.VMEM((groups, 8, LANES), F32),
        pltpu.VMEM(((ny + nz - 1) * 16, pw), BF16),
        pltpu.VMEM((t, d), BF16),
        pltpu.VMEM((4, width, t), BF16),
        pltpu.VMEM((2, width // 2, t), BF16),
        pltpu.VMEM((nz, ny * 32, t), F32),
        pltpu.VMEM((d // LANES, LANES), BF16),
        pltpu.VMEM(conv_taps.shape, BF16),
        pltpu.VMEM((1, width), F32),
        pltpu.VMEM(decay_shift.shape, F32),
        dma((10,)), dma((6,)), dma((6,)), dma((6,)), dma((6, 3)), dma((6,)),
        dma((6, 2, last, 2)), dma((6, 2, last, 2)), dma((6,)), dma((6,)), dma((6,)), dma((6,)), dma((6,)), dma((3,)), dma((4,)),
        dma((6,)), dma((6,)),
    ]
    return pl.pallas_call(
        functools.partial(body, nz, ny),
        out_shape=jax.ShapeDtypeStruct((t, d), BF16),
        in_specs=[any_] * 10,
        out_specs=any_,
        scratch_shapes=scratch,
        compiler_params=pltpu.CompilerParams(
            collective_id=0, has_side_effects=True, vmem_limit_bytes=60 * 1024 * 1024
        ),
        name="recurrence",
    )(
        tokens, norm_gain.reshape(-1, LANES), proj_x, gate_projection, conv_taps, gate_recur, gate_input,
        decay_param.reshape(1, -1), decay_shift, jnp.transpose(proj_out),
    )


def build(mesh, nz, ny):
    split = Mesh(mesh.devices.reshape(nz, ny, 2, mesh.shape["tp"]), ("sp_0", "sp_1", "sp_2", "tp"))
    in_specs = (
        P(SP_TP, None),
        P(),
        P(SP, "tp"),
        P(SP, "tp"),
        P(None, "tp"),
        P("tp", None, None),
        P("tp", None, None),
        P("tp"),
        P("tp", SP),
        P("tp", SP),
    )
    out_specs = P(SP_TP, None)
    return jax.shard_map(
        functools.partial(on_device, nz, ny), mesh=split, in_specs=in_specs, out_specs=out_specs, check_vma=False
    )


def solution(mesh):
    return build(mesh, 8, 8)
```
